256 devices in a mesh: ep: 64 (over z, y, core), tp: 4 (over x).
Axes of the slice: x: 4, y: 4, z: 8, core: 2. Of those that a mesh axis runs over, the one named last changes fastest.
Arguments:
- queries: bfloat16 [16384, 768], P('ep', 'tp'), may hold values from -270 to 270
- key_rows: bfloat16 [16384, 256], P('ep', 'tp'), may hold values from -6 to 6
- value_rows: bfloat16 [16384, 256], P('ep', 'tp'), may hold values from -6 to 6
- sink_logits: float32 [12], P('tp'), may hold values from 2 to 6
- out_weight: bfloat16 [768, 2048], P('tp'), may hold values from -0.21875 to 0.21875
- mix_gain: float32 [2048], replicated, may hold values from 0.1 to 1.9
- moe_tokens: bfloat16 [32768, 2048], P(('ep', 'tp')), may hold values from -600 to 600
- moe_gain: float32 [2048], replicated, may hold values from 0.1 to 1.9
- routes: int32 [32768, 2], P(('ep', 'tp')), may hold values from 0 to 63, all different within a row; in each aligned block of 128 rows (0 to 127, 128 to 255, ...) at most 5 rows name the same one
- route_weights: float32 [32768, 2], P(('ep', 'tp')), may hold values from 0.25 to 1.5
- expert_gate: bfloat16 [64, 2048, 3584], P('ep', None, 'tp'), may hold values from -0.125 to 0.125
- expert_up: bfloat16 [64, 2048, 3584], P('ep', None, 'tp'), may hold values from -0.125 to 0.125
- expert_down: bfloat16 [64, 3584, 2048], P('ep', 'tp'), may hold values from -0.09375 to 0.09375
Outputs:
- mixed: bfloat16 [16384, 2048], P(('ep', 'tp'))
- moe_out: bfloat16 [32768, 2048], P(('ep', 'tp'))
The draws below stay inside these ranges and needn't reach their ends.
Inputs may be any that keep to these rules, and one draw needn't show every extreme that they name: `routes`: each row names 2 different experts. In the rows of one device no expert is named more than 5 times, and in every draw some device names some expert exactly 5 times.
All inputs are finite; a program needn't handle non-finite values.
Results may differ from the reference program's by a relative error of at most 0.012.
Values may be sent and summed in bfloat16 or wider, within the bound.
A program may use at most 128 MiB of HBM per device.

```python
import math
import jax
import jax.numpy as jnp
import numpy as np
from jax import lax

D = 2048
FF = 3584
HEADS = 12
KV_HEADS = 4
HDIM = 64
GROUP = 3
WINDOW = 128
TOP = 2
TOK_EP = 256
ROWS_DEV = 128
TOKENS = 16384
ROWS = 32768
EXPERTS = 64
CAP = 5
N_EP = 64
N_TP = 4


def attention_draws(key):
    base = jax.random.fold_in(key, 4242)
    key_part = jnp.clip(jax.random.normal(jax.random.fold_in(base, 1), (TOKENS, KV_HEADS, HDIM), jnp.float32), -6.0, 6.0)
    query_part = jnp.clip(jax.random.normal(jax.random.fold_in(base, 2), (TOKENS, KV_HEADS, GROUP, HDIM), jnp.float32), -6.0, 6.0)
    return (key_part, query_part)


def draw_queries(key, part):
    key_part, query_part = attention_draws(key)
    return query_part.reshape(TOKENS, HEADS * HDIM).astype(jnp.bfloat16)


def draw_key_rows(key, part):
    key_part, query_part = attention_draws(key)
    return key_part.reshape(TOKENS, KV_HEADS * HDIM).astype(jnp.bfloat16)


def draw_moe_tokens(key, part):
    base = jax.random.fold_in(key, 5151)
    tokens_draw = jnp.clip(jax.random.normal(jax.random.fold_in(base, 1), (ROWS, D), jnp.float32), -6.0, 6.0)
    return tokens_draw.astype(jnp.bfloat16)


def block_scale(own_key, shape, shards, least, high):
    def one(dim, shards_of):
        draws = jax.random.uniform(jax.random.fold_in(jax.random.fold_in(own_key, 6), dim), (shards_of,), jnp.float32, least / len(shards), high / len(shards))
        return jnp.repeat(jnp.exp(draws), shape[dim] // shards_of).reshape((-1,) + (1,) * (len(shape) - dim - 1))

    loudness = one(*shards[0])
    for cut in shards[1:]:
        loudness = loudness * one(*cut)
    return loudness


def assign_block(stream_key, own, number, rows, count, top, bound, skew):
    sequence = jax.random.permutation(stream_key, count)
    heavy_load, common = load_shares(count, rows * top, bound, skew, True), load_shares(count, rows * top, bound, skew, False)
    places = jnp.arange(count)

    def named(lengths, turn):
        used = int((lengths > 0).sum())
        fixed = max(1, used // 4)
        moved = fixed + (places - fixed + turn * (used - fixed)) % max(1, count - fixed)
        return jnp.zeros((count,), jnp.int32).at[sequence[jnp.where(places < fixed, places, moved)]].set(jnp.asarray(lengths, jnp.int32))

    lengths = jnp.where(number % 4 == 0, named(heavy_load, number // 4), named(common, number - number // 4 - 1))
    mixed = jax.random.permutation(jax.random.fold_in(own, 3), count)
    source_of, receiver = mixed[0:count // 2 * 2:2], mixed[1:count // 2 * 2:2]
    margin = jnp.minimum(lengths[source_of] - 1, bound - lengths[receiver]) // 2
    margin = jnp.where((source_of == sequence[0]) | (receiver == sequence[0]) | (lengths[receiver] == 0), 0, jnp.maximum(margin, 0))
    moved = jax.random.randint(jax.random.fold_in(own, 4), (count // 2,), 0, 1 << 20) % (margin + 1)
    lengths = lengths.at[source_of].add(-moved).at[receiver].add(moved)
    items = jnp.searchsorted(jnp.cumsum(lengths), jnp.arange(rows * top), side="right").astype(jnp.int32)
    grid = items.reshape(top, rows).T
    grid = grid[jax.random.permutation(jax.random.fold_in(own, 1), rows)]
    turn = jax.random.randint(jax.random.fold_in(own, 2), (rows, 1), 0, top)
    return jnp.take_along_axis(grid, (jnp.arange(top)[None, :] + turn) % top, axis=1)


def load_shares(count, total, reach, skew, full):
    portions = [(1 << 20) // math.isqrt(standing ** skew) + 1 for standing in range(1, count + 1)]
    largest = reach if full else min(reach, max(-(-total // count), total * portions[0] // sum(portions)))
    least = 1 if total - largest >= count - 1 else 0
    given, rest = [largest] + [least] * (count - 1), total - largest - least * (count - 1)
    while rest > 0:
        candidates = [i for i in range(1, count) if given[i] < largest] or [i for i in range(1, count) if given[i] < reach]
        mass, remaining = sum([portions[i] for i in candidates]), rest
        for i in candidates:
            extra = min(reach - given[i], max(1, remaining * portions[i] // mass), rest)
            given[i] = given[i] + extra
            rest = rest - extra
    return np.array(given)


def gaussian(stream_key, dims, width, most, cuts=(), held_as=jnp.bfloat16):
    result = jax.random.normal(stream_key, dims, jnp.float32) * width
    if len(cuts) > 0:
        result = block_scale(stream_key, dims, cuts, -0.22, 0.18) * result
    return jnp.clip(result, min=-most, max=most).astype(held_as)


def setup_inputs(seed: int = 0) -> dict:
    arg_keys = jax.random.split(jax.random.key(seed), 14)
    queries = draw_queries(jax.random.fold_in(arg_keys[13], 71), 0)
    key_rows = draw_key_rows(jax.random.fold_in(arg_keys[13], 71), 0)
    value_rows = gaussian(arg_keys[2], (TOKENS, KV_HEADS * HDIM), 1.0, 6.0, ((0, 64), (1, 4)))
    sink_logits = jnp.clip(2.0 + 4.0 * jax.random.uniform(arg_keys[3], (HEADS,), jnp.float32) ** block_scale(arg_keys[3], (HEADS,), ((0, 4),), -0.2, 0.2), 2.0, 6.0)
    out_weight = gaussian(arg_keys[4], (HEADS * HDIM, D), (HEADS * HDIM) ** -0.5, 0.21875, ((0, 4),))
    mix_gain = jnp.clip(1.0 + 0.18 * jax.random.normal(arg_keys[5], (D,), jnp.float32), 0.1, 1.9)
    moe_tokens = draw_moe_tokens(jax.random.fold_in(arg_keys[13], 71), 0)
    moe_gain = jnp.clip(1.0 + 0.18 * jax.random.normal(arg_keys[7], (D,), jnp.float32), 0.1, 1.9)
    routes_keys = jax.random.split(jax.random.fold_in(arg_keys[8], 1), ROWS // ROWS_DEV)
    routes_turns = jax.random.permutation(jax.random.fold_in(arg_keys[8], 3), ROWS // ROWS_DEV)
    routes = jax.vmap(lambda own, number: assign_block(jax.random.fold_in(arg_keys[8], 2), own, number, ROWS_DEV, EXPERTS, TOP, CAP, 0))(routes_keys, routes_turns).reshape((ROWS, TOP))
    route_weights = jnp.clip(jnp.exp(math.log(1.5) - 1.7917595 * jax.random.uniform(arg_keys[9], (ROWS, TOP), jnp.float32) ** block_scale(arg_keys[9], (ROWS, TOP), ((0, 256),), -0.2, 0.2)), 0.25, 1.5)
    expert_gate = gaussian(arg_keys[10], (EXPERTS, D, FF), D ** -0.5, 0.125, ((0, 64), (2, 4)))
    expert_up = gaussian(arg_keys[11], (EXPERTS, D, FF), D ** -0.5, 0.125, ((0, 64), (2, 4)))
    expert_down = gaussian(arg_keys[12], (EXPERTS, FF, D), FF ** -0.5, 0.09375, ((0, 64), (1, 4)))
    return dict(queries=queries, key_rows=key_rows, value_rows=value_rows, sink_logits=sink_logits, out_weight=out_weight, mix_gain=mix_gain, moe_tokens=moe_tokens, moe_gain=moe_gain, routes=routes, route_weights=route_weights, expert_gate=expert_gate, expert_up=expert_up, expert_down=expert_down)


norm_eps = 1e-06
masked_value = -1e+30

def rms_scale(rows_in, gain):
    squares = lax.optimization_barrier(jnp.mean(rows_in * rows_in, axis=-1, keepdims=True))
    return rows_in * lax.rsqrt(squares + norm_eps) * gain

def reference(queries, key_rows, value_rows, sink_logits, out_weight, mix_gain, moe_tokens, moe_gain, routes, route_weights, expert_gate, expert_up, expert_down):
    head_cols = KV_HEADS * HDIM
    padded_keys = jnp.concatenate([jnp.zeros((WINDOW, head_cols), jnp.bfloat16), key_rows], axis=0)
    padded_values = jnp.concatenate([jnp.zeros((WINDOW, head_cols), jnp.bfloat16), value_rows], axis=0)

    def attend_block(block_index):
        first_row = (block_index * TOK_EP).astype(jnp.int32)
        block_queries = lax.dynamic_slice_in_dim(queries, first_row, TOK_EP, 0)
        block_keys = lax.dynamic_slice_in_dim(padded_keys, first_row, TOK_EP + WINDOW, 0)
        block_values = lax.dynamic_slice_in_dim(padded_values, first_row, TOK_EP + WINDOW, 0)
        query_pos = first_row + jnp.arange(TOK_EP, dtype=jnp.int32)
        key_pos = first_row - WINDOW + jnp.arange(TOK_EP + WINDOW, dtype=jnp.int32)
        distance = query_pos[:, None] - key_pos[None, :]
        allowed = (distance >= 0) & (distance < WINDOW) & (key_pos >= 0)[None, :]
        grouped = block_queries.reshape(TOK_EP, KV_HEADS, GROUP, HDIM).astype(jnp.float32)
        keys_f = block_keys.reshape(TOK_EP + WINDOW, KV_HEADS, HDIM).astype(jnp.float32)
        values_f = block_values.reshape(TOK_EP + WINDOW, KV_HEADS, HDIM).astype(jnp.float32)
        scores = jnp.einsum('qkgd,jkd->kgqj', grouped, keys_f) * HDIM ** (-0.5)
        logits = jnp.where(allowed, scores, masked_value)
        sink_logit = sink_logits.reshape(KV_HEADS, GROUP)[:, :, None, None]
        top_value = jnp.maximum(lax.optimization_barrier(jnp.max(logits, axis=-1, keepdims=True)), sink_logit)
        exponent = jnp.exp(logits - top_value)
        denominator = lax.optimization_barrier(jnp.sum(exponent, axis=-1, keepdims=True)) + jnp.exp(sink_logit - top_value)
        probs = (exponent / denominator).astype(jnp.bfloat16)
        attended = jnp.einsum('kgqj,jkd->qkgd', probs.astype(jnp.float32), values_f)
        return attended.astype(jnp.bfloat16).reshape(TOK_EP, HEADS * HDIM)
    attended = lax.map(attend_block, jnp.arange(N_EP, dtype=jnp.int32)).reshape(TOKENS, HEADS * HDIM)
    group_cols = HEADS * HDIM // N_TP
    projected = jnp.zeros((TOKENS, D), jnp.float32)
    for group_index in range(N_TP):
        lower = group_index * group_cols
        partial_value = jnp.dot(attended[:, lower:lower + group_cols], out_weight[lower:lower + group_cols], preferred_element_type=jnp.float32).astype(jnp.bfloat16)
        partial_value = lax.optimization_barrier(partial_value)
        projected = projected + partial_value.astype(jnp.float32)
    mixed = rms_scale(projected, mix_gain).astype(jnp.bfloat16)
    normed = rms_scale(moe_tokens.astype(jnp.float32), moe_gain).astype(jnp.bfloat16)
    slot_limit = N_EP * N_TP * CAP
    ff_block = FF // N_TP

    def expert_step(accumulated, inputs):
        gate_weight, up_weight, down_weight, expert_id = inputs
        chosen = routes == expert_id
        token_weight = lax.optimization_barrier(jnp.sum(jnp.where(chosen, route_weights, jnp.zeros_like(route_weights)), axis=1))
        member = jnp.any(chosen, axis=1)
        token_index = jnp.nonzero(member, size=slot_limit, fill_value=0)[0].astype(jnp.int32)
        valid_slot = jnp.arange(slot_limit, dtype=jnp.int32) < jnp.sum(member.astype(jnp.int32))
        slot_rows = normed[token_index]
        gate_value = jnp.dot(slot_rows, gate_weight, preferred_element_type=jnp.float32)
        up_value = jnp.dot(slot_rows, up_weight, preferred_element_type=jnp.float32)
        hidden = (jax.nn.silu(gate_value) * up_value).astype(jnp.bfloat16)
        summed = jnp.zeros((slot_limit, D), jnp.float32)
        for block_index in range(N_TP):
            lower = block_index * ff_block
            partial_value = jnp.dot(hidden[:, lower:lower + ff_block], down_weight[lower:lower + ff_block], preferred_element_type=jnp.float32).astype(jnp.bfloat16)
            partial_value = lax.optimization_barrier(partial_value)
            summed = summed + partial_value.astype(jnp.float32)
        expert_out = lax.optimization_barrier(summed.astype(jnp.bfloat16))
        row_weight = jnp.where(valid_slot, token_weight[token_index], jnp.zeros_like(token_weight[token_index]))
        accumulated = accumulated.at[token_index].add(row_weight[:, None] * expert_out.astype(jnp.float32))
        return (accumulated, None)
    combined, _ = lax.scan(expert_step, jnp.zeros((ROWS, D), jnp.float32), (expert_gate, expert_up, expert_down, jnp.arange(EXPERTS, dtype=jnp.int32)))
    return (mixed, combined.astype(jnp.bfloat16))
```

```python
import functools

import jax
import jax.numpy as jnp
from jax import lax
from jax.experimental import pallas as pl
from jax.experimental.pallas import tpu as pltpu
from jax.sharding import PartitionSpec as P

HDIM = 64
WINDOW = 128
MESH = pl.DeviceIdType.MESH

norm_eps = 1e-06
masked_value = -1e30

N_Z = 8
N_YC = 8
CAP = 5
CHUNKS = 4
HALVES = 2
OFFSETS = ((0, 1), (2, 6), (3, 5), (4, 7))
SELF_CHUNK = 0
ROWS = HALVES * N_YC * CAP
GROUPS = ROWS // 16
GROUP_ROWS = N_YC * CAP


def shifted(shard, axis, by):
    size = lax.axis_size(axis)
    pairs = [(i, i + by) for i in range(size) if 0 <= i + by < size]
    return lax.ppermute(shard, axis, pairs)


def rms_scale(rows_in, gain):
    squares = jnp.mean(rows_in * rows_in, axis=-1, keepdims=True)
    return rows_in * lax.rsqrt(squares + norm_eps) * gain


def mixer(queries, key_rows, value_rows, sink_logits, out_weight, mix_gain):
    tok_rows = queries.shape[0]
    kv_local = key_rows.shape[1] // HDIM
    group_size = queries.shape[1] // key_rows.shape[1]
    rim_rows = (key_rows[tok_rows - WINDOW :], value_rows[tok_rows - WINDOW :])
    prev_keys, prev_values = shifted((rim_rows[0], rim_rows[1]), "ep", 1)
    all_keys = jnp.concatenate([prev_keys, key_rows], axis=0).reshape(
        tok_rows + WINDOW, kv_local, HDIM
    )
    all_values = jnp.concatenate([prev_values, value_rows], axis=0).reshape(
        tok_rows + WINDOW, kv_local, HDIM
    )
    offset = lax.axis_index("ep") * tok_rows
    query_pos = offset + jnp.arange(tok_rows, dtype=jnp.int32)
    key_pos = offset - WINDOW + jnp.arange(tok_rows + WINDOW, dtype=jnp.int32)
    distance = query_pos[:, None] - key_pos[None, :]
    allowed = (distance >= 0) & (distance < WINDOW) & (key_pos >= 0)[None, :]
    grouped = queries.reshape(tok_rows, kv_local, group_size, HDIM)
    scores = jnp.einsum(
        "qkgd,jkd->kgqj", grouped, all_keys, preferred_element_type=jnp.float32
    ) * HDIM ** (-0.5)
    logits = jnp.where(allowed, scores, masked_value)
    sink_logit = sink_logits.reshape(kv_local, group_size)[:, :, None, None]
    top_value = jnp.maximum(jnp.max(logits, axis=-1, keepdims=True), sink_logit)
    exponent = jnp.exp(logits - top_value)
    denominator = jnp.sum(exponent, axis=-1, keepdims=True) + jnp.exp(sink_logit - top_value)
    probs = (exponent / denominator).astype(jnp.bfloat16)
    attended = jnp.einsum("kgqj,jkd->qkgd", probs, all_values, preferred_element_type=jnp.float32)
    attended = attended.astype(jnp.bfloat16).reshape(tok_rows, -1)
    projected = lax.psum_scatter(
        jnp.dot(attended, out_weight, preferred_element_type=jnp.float32).astype(jnp.bfloat16),
        "tp",
        scatter_dimension=0,
        tiled=True,
    ).astype(jnp.float32)
    return rms_scale(projected, mix_gain).astype(jnp.bfloat16)


def pick(index, table):
    value = jnp.int32(table[-1])
    for place in range(len(table) - 2, -1, -1):
        value = jnp.where(index == place, jnp.int32(table[place]), value)
    return value


def rows_to_tiles(block, perm, width):
    lanes = width // 16
    stacked = jnp.concatenate(
        [
            jnp.concatenate(
                [block[16 * g : 16 * g + 16, lanes * s : lanes * s + lanes] for s in range(16)],
                axis=0,
            )
            for g in range(GROUPS)
        ],
        axis=1,
    )
    turned = jnp.dot(perm, stacked, preferred_element_type=jnp.float32).astype(jnp.bfloat16)
    return [turned[:, lanes * g : lanes * g + lanes].reshape(16, 16, lanes) for g in range(GROUPS)]


def tiles_to_rows(tiles, perm, lanes):
    stacked = jnp.concatenate(
        [tiles[16 * g : 16 * g + 16].reshape(256, lanes) for g in range(GROUPS)], axis=1
    )
    turned = jnp.dot(perm, stacked, preferred_element_type=jnp.float32).astype(jnp.bfloat16)
    return [
        [turned[16 * s : 16 * s + 16, lanes * g : lanes * g + lanes] for s in range(16)]
        for g in range(GROUPS)
    ]


def experts_kernel(
    n_tp,
    tokens_ref,
    gain_ref,
    routes_ref,
    weights_ref,
    gate_ref,
    up_ref,
    down_ref,
    out_ref,
    outb,
    recv,
    xbuf,
    pbuf,
    r1,
    r2,
    back,
    ret,
    wgu,
    wdn,
    hid,
    acc,
    mix,
    perm_ref,
    row_ref,
    w_sem,
    a_send,
    a_recv,
    g_send,
    g_recv,
    q_send,
    q_recv,
    b_send,
    b_recv,
):
    width = tokens_ref.shape[1]
    half = width // 2
    lanes = width // 16
    gate_tiles = wgu.shape[0]
    down_tiles = wdn.shape[0]
    me = lax.axis_index("ep")
    tp = lax.axis_index("tp")
    z = lax.div(me, jnp.int32(N_YC))
    yc = lax.rem(me, jnp.int32(N_YC))
    right = lax.rem(tp + 1, jnp.int32(n_tp))
    left = lax.rem(tp + n_tp - 1, jnp.int32(n_tp))

    barrier = pltpu.get_barrier_semaphore()

    def greet(i, carry):
        @pl.when(i != me)
        def _():
            pl.semaphore_signal(barrier, inc=1, device_id={"ep": i}, device_id_type=MESH)

        return carry

    lax.fori_loop(0, N_Z * N_YC, greet, 0)
    pl.semaphore_signal(barrier, inc=1, device_id={"tp": right}, device_id_type=MESH)
    pl.semaphore_signal(barrier, inc=1, device_id={"tp": left}, device_id_type=MESH)

    for n in range(gate_tiles):
        for part, ref in enumerate((gate_ref, up_ref)):
            pltpu.make_async_copy(
                ref.at[0, :, pl.ds(128 * n, 128)], wgu.at[n, :, pl.ds(128 * part, 128)], w_sem.at[0]
            ).start()
    for n in range(down_tiles):
        pltpu.make_async_copy(
            down_ref.at[0, :, pl.ds(256 * n, 256)], wdn.at[n], w_sem.at[1]
        ).start()

    tok = tokens_ref.shape[0]
    e_rows = [routes_ref[0:1, :], routes_ref[1:2, :]]
    expert_id = lax.broadcasted_iota(jnp.int32, (N_Z * N_YC, tok), 0)
    named = [jnp.where(expert_id == e, 1.0, 0.0) for e in e_rows]
    before = jnp.where(
        lax.broadcasted_iota(jnp.int32, (tok, tok), 0)
        < lax.broadcasted_iota(jnp.int32, (tok, tok), 1),
        1.0,
        0.0,
    ).astype(jnp.bfloat16)
    ranks = [
        jnp.dot(n.astype(jnp.bfloat16), before, preferred_element_type=jnp.float32) for n in named
    ]
    ranks[1] = ranks[1] + jnp.sum(named[0], axis=1, keepdims=True)
    slots = []
    flat_offsets = [o for pair in OFFSETS for o in pair]
    for e, n, r in zip(e_rows, named, ranks):
        rank = jnp.sum(n * r, axis=0, keepdims=True).astype(jnp.int32)
        offset = (lax.shift_right_logical(e, 3) - z) & (N_Z - 1)
        place = jnp.zeros_like(offset)
        for p, o in enumerate(flat_offsets):
            place = jnp.where(offset == o, p, place)
        slots.append((place * N_YC + (e & (N_YC - 1))) * CAP + rank)

    i256 = lax.broadcasted_iota(jnp.int32, (256, 256), 0)
    j256 = lax.broadcasted_iota(jnp.int32, (256, 256), 1)
    perm_ref[...] = jnp.where(
        j256 == (i256 & 15) * 16 + lax.shift_right_logical(i256, 4), 1.0, 0.0
    ).astype(jnp.bfloat16)

    x = tokens_ref[...].astype(jnp.float32)
    squares = jnp.mean(x * x, axis=-1, keepdims=True)
    row_ref[...] = (x * lax.rsqrt(squares + norm_eps) * gain_ref[...]).astype(jnp.bfloat16)

    def peer(i, y, sign, k):
        distance = pick(k, [pair[i] for pair in OFFSETS])
        return lax.rem(z + sign * distance + N_Z, jnp.int32(N_Z)) * N_YC + y

    def a_copy(k, i, y):
        return pltpu.make_async_remote_copy(
            src_ref=outb.at[k, i * N_YC + y],
            dst_ref=recv.at[k, i * N_YC + yc],
            send_sem=a_send.at[k],
            recv_sem=a_recv.at[k],
            device_id={"ep": peer(i, y, 1, k)},
            device_id_type=MESH,
        )

    def b_copy(k, i, y):
        return pltpu.make_async_remote_copy(
            src_ref=back.at[k, i * N_YC + y],
            dst_ref=ret.at[k, i * N_YC + yc],
            send_sem=b_send.at[k],
            recv_sem=b_recv.at[k],
            device_id={"ep": peer(i, y, -1, k)},
            device_id_type=MESH,
        )

    def spread(copy_of, k):
        def one(y, carry):
            for i in range(HALVES):
                if i == 0:

                    @pl.when(jnp.logical_not(jnp.logical_and(k == SELF_CHUNK, y == yc)))
                    def _():
                        copy_of(k, 0, y).start()
                else:
                    copy_of(k, i, y).start()
            return carry

        lax.fori_loop(0, N_YC, one, 0)

    def bulk(buffer, sem, k):
        @pl.when(k == SELF_CHUNK)
        def _():
            view = buffer.at[k, pl.ds(0, HALVES * N_YC - 1)]
            pltpu.make_async_copy(view, view, sem.at[k]).wait()

        @pl.when(k != SELF_CHUNK)
        def _():
            view = buffer.at[k]
            pltpu.make_async_copy(view, view, sem.at[k]).wait()

    def dispatch(k, carry):
        row_id = lax.broadcasted_iota(jnp.int32, (ROWS, tok), 0) + k * ROWS
        hits = [row_id == s for s in slots]
        select = jnp.where(jnp.logical_or(hits[0], hits[1]), 1.0, 0.0).astype(jnp.bfloat16)
        shares = jnp.where(hits[0], weights_ref[0:1, :], 0.0) + jnp.where(
            hits[1], weights_ref[1:2, :], 0.0
        )
        coarse = shares.astype(jnp.bfloat16)
        mix[k, 0] = coarse
        mix[k, 1] = (shares - coarse.astype(jnp.float32)).astype(jnp.bfloat16)
        block = jnp.dot(select, row_ref[...], preferred_element_type=jnp.float32)
        tiles = rows_to_tiles(block.astype(jnp.bfloat16), perm_ref[...], width)
        flat = outb.at[k].reshape(ROWS, 16, lanes)
        for g in range(GROUPS):
            flat[16 * g : 16 * g + 16] = tiles[g]

        @pl.when(k == 0)
        def _():
            pl.semaphore_wait(barrier, N_Z * N_YC - 1 + 2)

        @pl.when(k == SELF_CHUNK)
        def _():
            recv[k, yc] = outb[k, yc]

        spread(a_copy, k)
        return carry

    lax.fori_loop(0, CHUNKS, dispatch, 0)
    acc[...] = jnp.zeros_like(acc)

    low = pl.ds(0, half)
    high = pl.ds(half, half)

    def g_copy(k, which):
        if which == 0:
            src, dst, to = xbuf.at[k, 0], xbuf.at[k, 1], right
        elif which == 1:
            src, dst, to = xbuf.at[k, 0], xbuf.at[k, 2], left
        elif which == 2:
            src, dst, to = xbuf.at[k, 1, :, low], xbuf.at[k, 3, :, low], right
        else:
            src, dst, to = xbuf.at[k, 2, :, high], xbuf.at[k, 3, :, high], left
        return pltpu.make_async_remote_copy(
            src_ref=src,
            dst_ref=dst,
            send_sem=g_send.at[k, which],
            recv_sem=g_recv.at[k, which],
            device_id={"tp": to},
            device_id_type=MESH,
        )

    def q_copy(k, which):
        if which == 0:
            src, dst, to = pbuf.at[k, 3, :, low], r1.at[k, 0], right
        elif which == 1:
            src, dst, to = pbuf.at[k, 3, :, high], r1.at[k, 1], left
        elif which == 2:
            src, dst, to = pbuf.at[k, 2, :, high], r2.at[k, 0, :, high], right
        elif which == 3:
            src, dst, to = pbuf.at[k, 1, :, low], r2.at[k, 1, :, low], left
        elif which == 4:
            src, dst, to = pbuf.at[k, 2, :, low], r2.at[k, 0, :, low], right
        else:
            src, dst, to = pbuf.at[k, 1, :, high], r2.at[k, 1, :, high], left
        return pltpu.make_async_remote_copy(
            src_ref=src,
            dst_ref=dst,
            send_sem=q_send.at[k, which],
            recv_sem=q_recv.at[k, which],
            device_id={"tp": to},
            device_id_type=MESH,
        )

    def arrive(k):
        bulk(recv, a_recv, k)
        rows = tiles_to_rows(recv[k].reshape(ROWS, 16, lanes), perm_ref[...], lanes)
        for g in range(GROUPS):
            for s in range(16):
                xbuf[k, 0, 16 * g : 16 * g + 16, lanes * s : lanes * s + lanes] = rows[g][s]
        g_copy(k, 0).start()
        g_copy(k, 1).start()

    def forward(k):
        g_copy(k, 0).wait_recv()
        g_copy(k, 2).start()
        g_copy(k, 1).wait_recv()
        g_copy(k, 3).start()

    def multiply(k):
        @pl.when(k == 0)
        def _():
            pltpu.make_async_copy(wgu, wgu, w_sem.at[0]).wait()
            pltpu.make_async_copy(wdn, wdn, w_sem.at[1]).wait()

        g_copy(k, 2).wait_recv()
        g_copy(k, 3).wait_recv()
        for n in range(gate_tiles):
            both = jnp.dot(
                xbuf[k].reshape(n_tp * ROWS, width), wgu[n], preferred_element_type=jnp.float32
            )
            gate, up = both[:, :128], both[:, 128:]
            hid[:, 128 * n : 128 * n + 128] = (gate / (1.0 + jnp.exp(-gate)) * up).astype(
                jnp.bfloat16
            )
        for n in range(down_tiles):
            part = jnp.dot(hid[...], wdn[n], preferred_element_type=jnp.float32)
            pbuf[k, :, :, 256 * n : 256 * n + 256] = part.astype(jnp.bfloat16).reshape(
                n_tp, ROWS, 256
            )
        for which in range(4):
            q_copy(k, which).start()

    def relay(k):
        q_copy(k, 0).wait_recv()
        pbuf[k, 2, :, low] = (
            pbuf[k, 2, :, low].astype(jnp.float32) + r1[k, 0].astype(jnp.float32)
        ).astype(jnp.bfloat16)
        q_copy(k, 4).start()
        q_copy(k, 1).wait_recv()
        pbuf[k, 1, :, high] = (
            pbuf[k, 1, :, high].astype(jnp.float32) + r1[k, 1].astype(jnp.float32)
        ).astype(jnp.bfloat16)
        q_copy(k, 5).start()

    def finish(k):
        for which in range(2, 6):
            q_copy(k, which).wait_recv()
        total = (
            pbuf[k, 0].astype(jnp.float32)
            + r2[k, 0].astype(jnp.float32)
            + r2[k, 1].astype(jnp.float32)
        ).astype(jnp.bfloat16)
        tiles = rows_to_tiles(total, perm_ref[...], width)
        flat = back.at[k].reshape(ROWS, 16, lanes)
        for g in range(GROUPS):
            flat[16 * g : 16 * g + 16] = tiles[g]

        @pl.when(k == SELF_CHUNK)
        def _():
            ret[k, yc] = back[k, yc]

        spread(b_copy, k)

    def combine(k):
        bulk(ret, b_recv, k)
        rows = tiles_to_rows(ret[k].reshape(ROWS, 16, lanes), perm_ref[...], lanes)
        block = jnp.concatenate([jnp.concatenate(r, axis=1) for r in rows], axis=0)
        dims = (((0,), (0,)), ((), ()))
        acc[...] += lax.dot_general(
            mix[k, 0], block, dims, preferred_element_type=jnp.float32
        ) + lax.dot_general(mix[k, 1], block, dims, preferred_element_type=jnp.float32)

    stages = ((arrive, 0), (forward, 1), (multiply, 2), (relay, 3), (finish, 4), (combine, 5))

    def step(s, carry):
        for stage, lag in stages:

            @pl.when(jnp.logical_and(s >= lag, s < lag + CHUNKS))
            def _(stage=stage, lag=lag):
                stage(s - lag)

        return carry

    lax.fori_loop(0, CHUNKS + 5, step, 0)
    out_ref[...] = acc[...].astype(jnp.bfloat16)

    def drain(k, carry):
        bulk(outb, a_send, k)
        bulk(back, b_send, k)
        for which in range(4):
            g_copy(k, which).wait_send()
        for which in range(6):
            q_copy(k, which).wait_send()
        return carry

    lax.fori_loop(0, CHUNKS, drain, 0)


def routed_experts(
    moe_tokens, moe_gain, routes, route_weights, expert_gate, expert_up, expert_down
):
    tok, width = moe_tokens.shape
    n_tp = lax.axis_size("tp")
    hidden = expert_gate.shape[2]
    lanes = width // 16
    bf16 = jnp.bfloat16
    vmem = pl.BlockSpec(memory_space=pltpu.VMEM)
    hbm = pl.BlockSpec(memory_space=pl.ANY)
    tiles = (CHUNKS, HALVES * N_YC, CAP, 16, lanes)
    return pl.pallas_call(
        functools.partial(experts_kernel, n_tp),
        out_shape=jax.ShapeDtypeStruct((tok, width), bf16),
        in_specs=[vmem, vmem, vmem, vmem, hbm, hbm, hbm],
        out_specs=vmem,
        scratch_shapes=[
            pltpu.VMEM(tiles, bf16),
            pltpu.VMEM(tiles, bf16),
            pltpu.VMEM((CHUNKS, n_tp, ROWS, width), bf16),
            pltpu.VMEM((CHUNKS, n_tp, ROWS, width), bf16),
            pltpu.VMEM((CHUNKS, 2, ROWS, width // 2), bf16),
            pltpu.VMEM((CHUNKS, 2, ROWS, width), bf16),
            pltpu.VMEM(tiles, bf16),
            pltpu.VMEM(tiles, bf16),
            pltpu.VMEM((hidden // 128, width, 256), bf16),
            pltpu.VMEM((width // 256, hidden, 256), bf16),
            pltpu.VMEM((n_tp * ROWS, hidden), bf16),
            pltpu.VMEM((tok, width), jnp.float32),
            pltpu.VMEM((CHUNKS, 2, ROWS, tok), bf16),
            pltpu.VMEM((256, 256), bf16),
            pltpu.VMEM((tok, width), bf16),
            pltpu.SemaphoreType.DMA((2,)),
            pltpu.SemaphoreType.DMA((CHUNKS,)),
            pltpu.SemaphoreType.DMA((CHUNKS,)),
            pltpu.SemaphoreType.DMA((CHUNKS, 4)),
            pltpu.SemaphoreType.DMA((CHUNKS, 4)),
            pltpu.SemaphoreType.DMA((CHUNKS, 6)),
            pltpu.SemaphoreType.DMA((CHUNKS, 6)),
            pltpu.SemaphoreType.DMA((CHUNKS,)),
            pltpu.SemaphoreType.DMA((CHUNKS,)),
        ],
        compiler_params=pltpu.CompilerParams(
            collective_id=0, has_side_effects=True, vmem_limit_bytes=56 * 1024 * 1024
        ),
        cost_estimate=pl.CostEstimate(
            flops=2 * 3 * CHUNKS * n_tp * ROWS * width * hidden,
            bytes_accessed=3 * width * hidden * 2,
            transcendentals=0,
        ),
    )(
        moe_tokens,
        moe_gain[None, :],
        routes.T,
        route_weights.T,
        expert_gate,
        expert_up,
        expert_down,
    )


def shards(
    queries,
    key_rows,
    value_rows,
    sink_logits,
    out_weight,
    mix_gain,
    moe_tokens,
    moe_gain,
    routes,
    route_weights,
    expert_gate,
    expert_up,
    expert_down,
):
    mixed = mixer(queries, key_rows, value_rows, sink_logits, out_weight, mix_gain)
    moe_out = routed_experts(
        moe_tokens, moe_gain, routes, route_weights, expert_gate, expert_up, expert_down
    )
    return (mixed, moe_out)


def solution(mesh):
    return jax.shard_map(
        shards,
        mesh=mesh,
        in_specs=(
            P("ep", "tp"),
            P("ep", "tp"),
            P("ep", "tp"),
            P("tp"),
            P("tp", None),
            P(),
            P(("ep", "tp"), None),
            P(),
            P(("ep", "tp"), None),
            P(("ep", "tp"), None),
            P("ep", None, "tp"),
            P("ep", None, "tp"),
            P("ep", "tp", None),
        ),
        out_specs=(P(("ep", "tp"), None), P(("ep", "tp"), None)),
        check_vma=False,
    )
```

```python
import functools

import jax
import jax.numpy as jnp
from jax import lax
from jax.experimental import pallas as pl
from jax.experimental.pallas import tpu as pltpu
from jax.sharding import PartitionSpec as P

HDIM = 64
WINDOW = 128
MESH = pl.DeviceIdType.MESH

norm_eps = 1e-06
masked_value = -1e30

N_Z = 8
N_YC = 8
CAP = 5
CHUNKS = 4
HALVES = 2
OFFSETS = ((2, 6), (4, 7), (3, 5), (0, 1))
SELF_CHUNK = 3
ROWS = HALVES * N_YC * CAP
GROUPS = ROWS // 16


def pick(index, table):
    value = jnp.int32(table[-1])
    for place in range(len(table) - 2, -1, -1):
        value = jnp.where(index == place, jnp.int32(table[place]), value)
    return value


def rows_to_tiles(block, perm, width):
    lanes = width // 16
    stacked = jnp.concatenate(
        [
            jnp.concatenate(
                [block[16 * g : 16 * g + 16, lanes * s : lanes * s + lanes] for s in range(16)],
                axis=0,
            )
            for g in range(GROUPS)
        ],
        axis=1,
    )
    turned = jnp.dot(perm, stacked, preferred_element_type=jnp.float32).astype(jnp.bfloat16)
    return [turned[:, lanes * g : lanes * g + lanes].reshape(16, 16, lanes) for g in range(GROUPS)]


def tiles_to_rows(tiles, perm, lanes):
    stacked = jnp.concatenate(
        [tiles[16 * g : 16 * g + 16].reshape(256, lanes) for g in range(GROUPS)], axis=1
    )
    turned = jnp.dot(perm, stacked, preferred_element_type=jnp.float32).astype(jnp.bfloat16)
    return [
        [turned[16 * s : 16 * s + 16, lanes * g : lanes * g + lanes] for s in range(16)]
        for g in range(GROUPS)
    ]


def layer_kernel(
    n_tp,
    tokens_ref,
    gain_ref,
    routes_ref,
    weights_ref,
    queries_ref,
    keys_ref,
    values_ref,
    sink_ref,
    mix_gain_ref,
    gate_ref,
    up_ref,
    down_ref,
    project_ref,
    mixed_ref,
    out_ref,
    outb,
    recv,
    xbuf,
    pbuf,
    r1,
    r2,
    back,
    ret,
    wgu,
    wdn,
    hid,
    acc,
    mix,
    perm_ref,
    row_ref,
    halo,
    attended,
    wproj,
    mpart,
    m1,
    m2,
    h_send,
    h_recv,
    m_send,
    m_recv,
    w_sem,
    a_send,
    a_recv,
    g_send,
    g_recv,
    q_send,
    q_recv,
    b_send,
    b_recv,
):
    width = tokens_ref.shape[1]
    half = width // 2
    lanes = width // 16
    gate_tiles = wgu.shape[0]
    down_tiles = wdn.shape[0]
    me = lax.axis_index("ep")
    tp = lax.axis_index("tp")
    z = lax.div(me, jnp.int32(N_YC))
    yc = lax.rem(me, jnp.int32(N_YC))
    right = lax.rem(tp + 1, jnp.int32(n_tp))
    left = lax.rem(tp + n_tp - 1, jnp.int32(n_tp))

    barrier = pltpu.get_barrier_semaphore()

    def greet(i, carry):
        @pl.when(i != me)
        def _():
            pl.semaphore_signal(barrier, inc=1, device_id={"ep": i}, device_id_type=MESH)

        return carry

    lax.fori_loop(0, N_Z * N_YC, greet, 0)
    pl.semaphore_signal(barrier, inc=1, device_id={"tp": right}, device_id_type=MESH)
    pl.semaphore_signal(barrier, inc=1, device_id={"tp": left}, device_id_type=MESH)

    for n in range(gate_tiles):
        for part, ref in enumerate((gate_ref, up_ref)):
            pltpu.make_async_copy(
                ref.at[0, :, pl.ds(128 * n, 128)], wgu.at[n, :, pl.ds(128 * part, 128)], w_sem.at[0]
            ).start()
    for n in range(down_tiles):
        pltpu.make_async_copy(
            down_ref.at[0, :, pl.ds(256 * n, 256)], wdn.at[n], w_sem.at[1]
        ).start()

    pltpu.make_async_copy(project_ref, wproj, w_sem.at[2]).start()

    tok = tokens_ref.shape[0]
    e_rows = [routes_ref[0:1, :], routes_ref[1:2, :]]
    expert_id = lax.broadcasted_iota(jnp.int32, (N_Z * N_YC, tok), 0)
    named = [jnp.where(expert_id == e, 1.0, 0.0) for e in e_rows]
    before = jnp.where(
        lax.broadcasted_iota(jnp.int32, (tok, tok), 0)
        < lax.broadcasted_iota(jnp.int32, (tok, tok), 1),
        1.0,
        0.0,
    ).astype(jnp.bfloat16)
    ranks = [
        jnp.dot(n.astype(jnp.bfloat16), before, preferred_element_type=jnp.float32) for n in named
    ]
    ranks[1] = ranks[1] + jnp.sum(named[0], axis=1, keepdims=True)
    slots = []
    flat_offsets = [o for pair in OFFSETS for o in pair]
    for e, n, r in zip(e_rows, named, ranks):
        rank = jnp.sum(n * r, axis=0, keepdims=True).astype(jnp.int32)
        offset = (lax.shift_right_logical(e, 3) - z) & (N_Z - 1)
        place = jnp.zeros_like(offset)
        for p, o in enumerate(flat_offsets):
            place = jnp.where(offset == o, p, place)
        slots.append((place * N_YC + (e & (N_YC - 1))) * CAP + rank)

    i256 = lax.broadcasted_iota(jnp.int32, (256, 256), 0)
    j256 = lax.broadcasted_iota(jnp.int32, (256, 256), 1)
    perm_ref[...] = jnp.where(
        j256 == (i256 & 15) * 16 + lax.shift_right_logical(i256, 4), 1.0, 0.0
    ).astype(jnp.bfloat16)

    x = tokens_ref[...].astype(jnp.float32)
    squares = jnp.mean(x * x, axis=-1, keepdims=True)
    row_ref[...] = (x * lax.rsqrt(squares + norm_eps) * gain_ref[...]).astype(jnp.bfloat16)

    def peer(i, y, sign, k):
        distance = pick(k, [pair[i] for pair in OFFSETS])
        return lax.rem(z + sign * distance + N_Z, jnp.int32(N_Z)) * N_YC + y

    def a_copy(k, i, y):
        return pltpu.make_async_remote_copy(
            src_ref=outb.at[k, i * N_YC + y],
            dst_ref=recv.at[k, i * N_YC + yc],
            send_sem=a_send.at[k],
            recv_sem=a_recv.at[k],
            device_id={"ep": peer(i, y, 1, k)},
            device_id_type=MESH,
        )

    def b_copy(k, i, y):
        return pltpu.make_async_remote_copy(
            src_ref=back.at[k, i * N_YC + y],
            dst_ref=ret.at[k, i * N_YC + yc],
            send_sem=b_send.at[k],
            recv_sem=b_recv.at[k],
            device_id={"ep": peer(i, y, -1, k)},
            device_id_type=MESH,
        )

    def spread(copy_of, k):
        def one(y, carry):
            for i in range(HALVES):
                if i == 0:

                    @pl.when(jnp.logical_not(jnp.logical_and(k == SELF_CHUNK, y == yc)))
                    def _():
                        copy_of(k, 0, y).start()
                else:
                    copy_of(k, i, y).start()
            return carry

        lax.fori_loop(0, N_YC, one, 0)

    def bulk(buffer, sem, k):
        @pl.when(k == SELF_CHUNK)
        def _():
            view = buffer.at[k, pl.ds(0, HALVES * N_YC - 1)]
            pltpu.make_async_copy(view, view, sem.at[k]).wait()

        @pl.when(k != SELF_CHUNK)
        def _():
            view = buffer.at[k]
            pltpu.make_async_copy(view, view, sem.at[k]).wait()

    def dispatch(k, carry):
        row_id = lax.broadcasted_iota(jnp.int32, (ROWS, tok), 0) + k * ROWS
        hits = [row_id == s for s in slots]
        select = jnp.where(jnp.logical_or(hits[0], hits[1]), 1.0, 0.0).astype(jnp.bfloat16)
        shares = jnp.where(hits[0], weights_ref[0:1, :], 0.0) + jnp.where(
            hits[1], weights_ref[1:2, :], 0.0
        )
        coarse = shares.astype(jnp.bfloat16)
        mix[k, 0] = coarse
        mix[k, 1] = (shares - coarse.astype(jnp.float32)).astype(jnp.bfloat16)
        block = jnp.dot(select, row_ref[...], preferred_element_type=jnp.float32)
        tiles = rows_to_tiles(block.astype(jnp.bfloat16), perm_ref[...], width)
        flat = outb.at[k].reshape(ROWS, 16, lanes)
        for g in range(GROUPS):
            flat[16 * g : 16 * g + 16] = tiles[g]

        return carry

    with jax.named_scope("dispatch"):
        lax.fori_loop(0, CHUNKS, dispatch, 0)
    with jax.named_scope("barrier_wait"):
        pl.semaphore_wait(barrier, N_Z * N_YC - 1 + 2)
    follower = lax.rem(me + 1, jnp.int32(N_Z * N_YC))

    def h_copy(which):
        ref = (keys_ref, values_ref)[which]
        return pltpu.make_async_remote_copy(
            src_ref=ref.at[:, pl.ds(ref.shape[1] - WINDOW, WINDOW)],
            dst_ref=halo.at[which],
            send_sem=h_send.at[which],
            recv_sem=h_recv.at[which],
            device_id={"ep": follower},
            device_id_type=MESH,
        )

    h_copy(0).start()
    h_copy(1).start()
    recv[SELF_CHUNK, yc] = outb[SELF_CHUNK, yc]

    def send(k, carry):
        spread(a_copy, k)
        return carry

    with jax.named_scope("send"):
        lax.fori_loop(0, CHUNKS, send, 0)
    acc[...] = jnp.zeros_like(acc)

    heads = queries_ref.shape[0] // HDIM
    sinks = jnp.concatenate(
        [jnp.full((1, WINDOW), sink_ref[h], jnp.float32) for h in range(heads)], axis=1
    )
    key_i = lax.broadcasted_iota(jnp.int32, (2 * WINDOW, heads * WINDOW), 0)
    query_i = lax.broadcasted_iota(jnp.int32, (2 * WINDOW, heads * WINDOW), 1) & (WINDOW - 1)
    in_window = jnp.logical_and(key_i > query_i, key_i <= query_i + WINDOW)

    def attend(b, keys, values, allowed):
        at = slice(WINDOW * b, WINDOW * b + WINDOW)
        block = jnp.concatenate(
            [queries_ref[HDIM * h : HDIM * h + HDIM, at] for h in range(heads)], axis=1
        )
        scores = lax.dot_general(
            keys, block, (((0,), (0,)), ((), ())), preferred_element_type=jnp.float32
        ) * HDIM ** (-0.5)
        logits = jnp.where(allowed, scores, masked_value)
        top = jnp.maximum(jnp.max(logits, axis=0, keepdims=True), sinks)
        exponent = jnp.exp(logits - top)
        denominator = jnp.sum(exponent, axis=0, keepdims=True) + jnp.exp(sinks - top)
        probs = (exponent / denominator).astype(jnp.bfloat16)
        result = jnp.dot(values, probs, preferred_element_type=jnp.float32).astype(jnp.bfloat16)
        for h in range(heads):
            attended[HDIM * h : HDIM * h + HDIM, at] = result[:, WINDOW * h : WINDOW * h + WINDOW]

    blocks = queries_ref.shape[1] // WINDOW
    with jax.named_scope("attend_own"):
        for b in range(1, blocks):
            at = slice(WINDOW * (b - 1), WINDOW * (b + 1))
            attend(b, keys_ref[:, at], values_ref[:, at], in_window)
    with jax.named_scope("halo_wait"):
        h_copy(0).wait_recv()
        h_copy(1).wait_recv()
    with jax.named_scope("attend_halo"):
        first = slice(0, WINDOW)
        attend(
            0,
            jnp.concatenate([halo[0], keys_ref[:, first]], axis=1),
            jnp.concatenate([halo[1], values_ref[:, first]], axis=1),
            jnp.logical_and(in_window, jnp.logical_or(key_i >= WINDOW, me > 0)),
        )
    with jax.named_scope("project"):
        pltpu.make_async_copy(wproj, wproj, w_sem.at[2]).wait()
        own_rows = mpart.shape[1]
        for n in range(width // 512):
            at = slice(512 * n, 512 * n + 512)
            part = lax.dot_general(
                attended[...],
                wproj[:, at],
                (((0,), (0,)), ((), ())),
                preferred_element_type=jnp.float32,
            ).astype(jnp.bfloat16)
            mpart[:, :, at] = part.reshape(n_tp, own_rows, 512)
    across = lax.rem(tp + 2, jnp.int32(n_tp))
    left_half = pl.ds(0, half)
    right_half = pl.ds(half, half)

    def m_copy(which):
        if which == 0:
            src, dst, to = mpart.at[across, :, left_half], m1.at[0], right
        elif which == 1:
            src, dst, to = mpart.at[across, :, right_half], m1.at[1], left
        elif which == 2:
            src, dst, to = mpart.at[right, :, right_half], m2.at[0, :, right_half], right
        elif which == 3:
            src, dst, to = mpart.at[left, :, left_half], m2.at[1, :, left_half], left
        elif which == 4:
            src, dst, to = mpart.at[right, :, left_half], m2.at[0, :, left_half], right
        else:
            src, dst, to = mpart.at[left, :, right_half], m2.at[1, :, right_half], left
        return pltpu.make_async_remote_copy(
            src_ref=src,
            dst_ref=dst,
            send_sem=m_send.at[which],
            recv_sem=m_recv.at[which],
            device_id={"tp": to},
            device_id_type=MESH,
        )

    for which in range(4):
        m_copy(which).start()

    def mixer_relay():
        m_copy(0).wait_recv()
        mpart[right, :, left_half] = (
            mpart[right, :, left_half].astype(jnp.float32) + m1[0].astype(jnp.float32)
        ).astype(jnp.bfloat16)
        m_copy(4).start()
        m_copy(1).wait_recv()
        mpart[left, :, right_half] = (
            mpart[left, :, right_half].astype(jnp.float32) + m1[1].astype(jnp.float32)
        ).astype(jnp.bfloat16)
        m_copy(5).start()

    def mixer_finish():
        for which in range(2, 6):
            m_copy(which).wait_recv()
        total = (
            mpart[tp].astype(jnp.float32)
            + m2[0].astype(jnp.float32)
            + m2[1].astype(jnp.float32)
        )
        squares = jnp.mean(total * total, axis=-1, keepdims=True)
        mixed_ref[...] = (total * lax.rsqrt(squares + norm_eps) * mix_gain_ref[...]).astype(
            jnp.bfloat16
        )

    low = pl.ds(0, half)
    high = pl.ds(half, half)

    def g_copy(k, which):
        if which == 0:
            src, dst, to = xbuf.at[k, 0], xbuf.at[k, 1], right
        elif which == 1:
            src, dst, to = xbuf.at[k, 0], xbuf.at[k, 2], left
        elif which == 2:
            src, dst, to = xbuf.at[k, 1, :, low], xbuf.at[k, 3, :, low], right
        else:
            src, dst, to = xbuf.at[k, 2, :, high], xbuf.at[k, 3, :, high], left
        return pltpu.make_async_remote_copy(
            src_ref=src,
            dst_ref=dst,
            send_sem=g_send.at[k, which],
            recv_sem=g_recv.at[k, which],
            device_id={"tp": to},
            device_id_type=MESH,
        )

    def q_copy(k, which):
        if which == 0:
            src, dst, to = pbuf.at[k, 3, :, low], r1.at[k, 0], right
        elif which == 1:
            src, dst, to = pbuf.at[k, 3, :, high], r1.at[k, 1], left
        elif which == 2:
            src, dst, to = pbuf.at[k, 2, :, high], r2.at[k, 0, :, high], right
        elif which == 3:
            src, dst, to = pbuf.at[k, 1, :, low], r2.at[k, 1, :, low], left
        elif which == 4:
            src, dst, to = pbuf.at[k, 2, :, low], r2.at[k, 0, :, low], right
        else:
            src, dst, to = pbuf.at[k, 1, :, high], r2.at[k, 1, :, high], left
        return pltpu.make_async_remote_copy(
            src_ref=src,
            dst_ref=dst,
            send_sem=q_send.at[k, which],
            recv_sem=q_recv.at[k, which],
            device_id={"tp": to},
            device_id_type=MESH,
        )

    def arrive(k):
        with jax.named_scope("arrive_wait"):
            bulk(recv, a_recv, k)
        rows = tiles_to_rows(recv[k].reshape(ROWS, 16, lanes), perm_ref[...], lanes)
        for g in range(GROUPS):
            for s in range(16):
                xbuf[k, 0, 16 * g : 16 * g + 16, lanes * s : lanes * s + lanes] = rows[g][s]
        g_copy(k, 0).start()
        g_copy(k, 1).start()

    def forward(k):
        with jax.named_scope("forward_wait"):
            g_copy(k, 0).wait_recv()
            g_copy(k, 2).start()
            g_copy(k, 1).wait_recv()
            g_copy(k, 3).start()

    def multiply(k):
        @pl.when(k == 0)
        def _():
            pltpu.make_async_copy(wgu, wgu, w_sem.at[0]).wait()
            pltpu.make_async_copy(wdn, wdn, w_sem.at[1]).wait()

        with jax.named_scope("multiply_wait"):
            g_copy(k, 2).wait_recv()
            g_copy(k, 3).wait_recv()
        for n in range(gate_tiles):
            both = jnp.dot(
                xbuf[k].reshape(n_tp * ROWS, width), wgu[n], preferred_element_type=jnp.float32
            )
            gate, up = both[:, :128], both[:, 128:]
            hid[:, 128 * n : 128 * n + 128] = (gate / (1.0 + jnp.exp(-gate)) * up).astype(
                jnp.bfloat16
            )
        for n in range(down_tiles):
            part = jnp.dot(hid[...], wdn[n], preferred_element_type=jnp.float32)
            pbuf[k, :, :, 256 * n : 256 * n + 256] = part.astype(jnp.bfloat16).reshape(
                n_tp, ROWS, 256
            )
        for which in range(4):
            q_copy(k, which).start()

    def relay(k):
        with jax.named_scope("relay_wait"):
            q_copy(k, 0).wait_recv()
        pbuf[k, 2, :, low] = (
            pbuf[k, 2, :, low].astype(jnp.float32) + r1[k, 0].astype(jnp.float32)
        ).astype(jnp.bfloat16)
        q_copy(k, 4).start()
        q_copy(k, 1).wait_recv()
        pbuf[k, 1, :, high] = (
            pbuf[k, 1, :, high].astype(jnp.float32) + r1[k, 1].astype(jnp.float32)
        ).astype(jnp.bfloat16)
        q_copy(k, 5).start()

    def finish(k):
        with jax.named_scope("finish_wait"):
            for which in range(2, 6):
                q_copy(k, which).wait_recv()
        total = (
            pbuf[k, 0].astype(jnp.float32)
            + r2[k, 0].astype(jnp.float32)
            + r2[k, 1].astype(jnp.float32)
        ).astype(jnp.bfloat16)
        tiles = rows_to_tiles(total, perm_ref[...], width)
        flat = back.at[k].reshape(ROWS, 16, lanes)
        for g in range(GROUPS):
            flat[16 * g : 16 * g + 16] = tiles[g]

        @pl.when(k == SELF_CHUNK)
        def _():
            ret[k, yc] = back[k, yc]

        spread(b_copy, k)

    def combine(k):
        with jax.named_scope("combine_wait"):
            bulk(ret, b_recv, k)
        rows = tiles_to_rows(ret[k].reshape(ROWS, 16, lanes), perm_ref[...], lanes)
        block = jnp.concatenate([jnp.concatenate(r, axis=1) for r in rows], axis=0)
        dims = (((0,), (0,)), ((), ()))
        acc[...] += lax.dot_general(
            mix[k, 0], block, dims, preferred_element_type=jnp.float32
        ) + lax.dot_general(mix[k, 1], block, dims, preferred_element_type=jnp.float32)

    stages = ((arrive, 0), (forward, 1), (multiply, 2), (relay, 3), (finish, 4), (combine, 5))

    def step(s, carry):
        for stage, lag in stages:
            if stage is forward:

                @pl.when(s == 0)
                def _():
                    with jax.named_scope("mixer_relay"):
                        mixer_relay()

                @pl.when(s == 3)
                def _():
                    with jax.named_scope("mixer_finish"):
                        mixer_finish()

            @pl.when(jnp.logical_and(s >= lag, s < lag + CHUNKS))
            def _(stage=stage, lag=lag):
                with jax.named_scope(stage.__name__):
                    stage(s - lag)

        return carry

    lax.fori_loop(0, CHUNKS + 5, step, 0)
    out_ref[...] = acc[...].astype(jnp.bfloat16)

    def drain(k, carry):
        bulk(outb, a_send, k)
        bulk(back, b_send, k)
        for which in range(4):
            g_copy(k, which).wait_send()
        for which in range(6):
            q_copy(k, which).wait_send()
        return carry

    with jax.named_scope("drain"):
        for which in range(2):
            h_copy(which).wait_send()
        for which in range(6):
            m_copy(which).wait_send()
        lax.fori_loop(0, CHUNKS, drain, 0)


def shards(
    queries,
    key_rows,
    value_rows,
    sink_logits,
    out_weight,
    mix_gain,
    moe_tokens,
    moe_gain,
    routes,
    route_weights,
    expert_gate,
    expert_up,
    expert_down,
):
    tok, width = moe_tokens.shape
    n_tp = lax.axis_size("tp")
    hidden = expert_gate.shape[2]
    lanes = width // 16
    own_rows = queries.shape[0] // n_tp
    bf16 = jnp.bfloat16
    vmem = pl.BlockSpec(memory_space=pltpu.VMEM)
    smem = pl.BlockSpec(memory_space=pltpu.SMEM)
    hbm = pl.BlockSpec(memory_space=pl.ANY)
    dma = pltpu.SemaphoreType.DMA
    tiles = (CHUNKS, HALVES * N_YC, CAP, 16, lanes)
    return pl.pallas_call(
        functools.partial(layer_kernel, n_tp),
        out_shape=(
            jax.ShapeDtypeStruct((own_rows, width), bf16),
            jax.ShapeDtypeStruct((tok, width), bf16),
        ),
        in_specs=[vmem] * 7 + [smem, vmem] + [hbm] * 4,
        out_specs=(vmem, vmem),
        scratch_shapes=[
            pltpu.VMEM(tiles, bf16),
            pltpu.VMEM(tiles, bf16),
            pltpu.VMEM((CHUNKS, n_tp, ROWS, width), bf16),
            pltpu.VMEM((CHUNKS, n_tp, ROWS, width), bf16),
            pltpu.VMEM((CHUNKS, 2, ROWS, width // 2), bf16),
            pltpu.VMEM((CHUNKS, 2, ROWS, width), bf16),
            pltpu.VMEM(tiles, bf16),
            pltpu.VMEM(tiles, bf16),
            pltpu.VMEM((hidden // 128, width, 256), bf16),
            pltpu.VMEM((width // 256, hidden, 256), bf16),
            pltpu.VMEM((n_tp * ROWS, hidden), bf16),
            pltpu.VMEM((tok, width), jnp.float32),
            pltpu.VMEM((CHUNKS, 2, ROWS, tok), bf16),
            pltpu.VMEM((256, 256), bf16),
            pltpu.VMEM((tok, width), bf16),
            pltpu.VMEM((2, HDIM, WINDOW), bf16),
            pltpu.VMEM((queries.shape[1], queries.shape[0]), bf16),
            pltpu.VMEM(out_weight.shape, bf16),
            pltpu.VMEM((n_tp, own_rows, width), bf16),
            pltpu.VMEM((2, own_rows, width // 2), bf16),
            pltpu.VMEM((2, own_rows, width), bf16),
            dma((2,)),
            dma((2,)),
            dma((6,)),
            dma((6,)),
            dma((3,)),
            dma((CHUNKS,)),
            dma((CHUNKS,)),
            dma((CHUNKS, 4)),
            dma((CHUNKS, 4)),
            dma((CHUNKS, 6)),
            dma((CHUNKS, 6)),
            dma((CHUNKS,)),
            dma((CHUNKS,)),
        ],
        compiler_params=pltpu.CompilerParams(
            collective_id=0, has_side_effects=True, vmem_limit_bytes=58 * 1024 * 1024
        ),
    )(
        moe_tokens,
        moe_gain[None, :],
        routes.T,
        route_weights.T,
        queries.T,
        key_rows.T,
        value_rows.T,
        sink_logits,
        mix_gain[None, :],
        expert_gate,
        expert_up,
        expert_down,
        out_weight,
    )


def solution(mesh):
    return jax.shard_map(
        shards,
        mesh=mesh,
        in_specs=(
            P("ep", "tp"),
            P("ep", "tp"),
            P("ep", "tp"),
            P("tp"),
            P("tp", None),
            P(),
            P(("ep", "tp"), None),
            P(),
            P(("ep", "tp"), None),
            P(("ep", "tp"), None),
            P("ep", None, "tp"),
            P("ep", None, "tp"),
            P("ep", "tp", None),
        ),
        out_specs=(P(("ep", "tp"), None), P(("ep", "tp"), None)),
        check_vma=False,
    )
```

```python
import functools

import jax
import jax.numpy as jnp
from jax import lax
from jax.experimental import pallas as pl
from jax.experimental.pallas import tpu as pltpu
from jax.sharding import PartitionSpec as P

HDIM = 64
WINDOW = 128
MESH = pl.DeviceIdType.MESH

norm_eps = 1e-06
masked_value = -1e30

N_Z = 8
N_YC = 8
CAP = 5
CHUNKS = 4
HALVES = 2
OFFSETS = ((2, 6), (4, 7), (3, 5), (0, 1))
SETTLE_ROWS = 64
SELF_CHUNK = 3
ORDER = (
    "D3 B S3 D0 S0 O D1 D2 H Q S1 A3 A0 S2 F3 A1 F0 M3 F1 A2 M0 W1 F2 L1 T0 M2 E1 L0 T2 E0 L2 T3 "
    "C1 E2 L3 P C0 E3 R C2 X C3"
)
ROWS = HALVES * N_YC * CAP
GROUPS = ROWS // 16


def rows_to_tiles(block, perm, width):
    lanes = width // 16
    stacked = jnp.concatenate(
        [
            jnp.concatenate(
                [block[16 * g : 16 * g + 16, lanes * s : lanes * s + lanes] for s in range(16)],
                axis=0,
            )
            for g in range(GROUPS)
        ],
        axis=1,
    )
    turned = jnp.dot(perm, stacked, preferred_element_type=jnp.float32).astype(jnp.bfloat16)
    return [turned[:, lanes * g : lanes * g + lanes].reshape(16, 16, lanes) for g in range(GROUPS)]


def tiles_to_rows(tiles, perm, lanes):
    stacked = jnp.concatenate(
        [tiles[16 * g : 16 * g + 16].reshape(256, lanes) for g in range(GROUPS)], axis=1
    )
    turned = jnp.dot(perm, stacked, preferred_element_type=jnp.float32).astype(jnp.bfloat16)
    return [
        [turned[16 * s : 16 * s + 16, lanes * g : lanes * g + lanes] for s in range(16)]
        for g in range(GROUPS)
    ]


def layer_kernel(
    n_tp,
    tokens_in,
    gain_in,
    routes_in,
    weights_in,
    queries_in,
    keys_in,
    values_in,
    sink_in,
    mix_gain_in,
    gate_ref,
    up_ref,
    down_ref,
    project_ref,
    mixed_out,
    moe_out,
    tokens_ref,
    gain_ref,
    routes_ref,
    weights_ref,
    queries_ref,
    keys_ref,
    values_ref,
    sink_ref,
    mix_gain_ref,
    mixed_ref,
    out_ref,
    outb,
    recv,
    xbuf,
    pbuf,
    r1,
    r2,
    back,
    ret,
    wgu,
    wdn,
    hid,
    acc,
    mix,
    perm_ref,
    row_ref,
    halo,
    attended,
    wproj,
    mpart,
    m1,
    m2,
    i_sem,
    o_sem,
    h_send,
    h_recv,
    m_send,
    m_recv,
    w_sem,
    a_send,
    a_recv,
    g_send,
    g_recv,
    q_send,
    q_recv,
    b_send,
    b_recv,
):
    width = tokens_ref.shape[1]
    half = width // 2
    lanes = width // 16
    gate_tiles = wgu.shape[0]
    down_tiles = wdn.shape[0]
    me = lax.axis_index("ep")
    tp = lax.axis_index("tp")
    z = lax.div(me, jnp.int32(N_YC))
    yc = lax.rem(me, jnp.int32(N_YC))
    right = lax.rem(tp + 1, jnp.int32(n_tp))
    left = lax.rem(tp + n_tp - 1, jnp.int32(n_tp))

    inputs = (
        (routes_in, routes_ref),
        (tokens_in, tokens_ref),
        (gain_in, gain_ref),
        (weights_in, weights_ref),
        (keys_in, keys_ref),
        (values_in, values_ref),
        (queries_in, queries_ref),
        (sink_in, sink_ref),
        (mix_gain_in, mix_gain_ref),
    )
    for n, (src, dst) in enumerate(inputs):
        pltpu.make_async_copy(src, dst, i_sem.at[n]).start()

    barrier = pltpu.get_barrier_semaphore()

    n_ep = N_Z * N_YC

    def greet(i, carry):
        other = lax.rem(me + n_ep // 2 + i, jnp.int32(n_ep))

        @pl.when(other != me)
        def _():
            pl.semaphore_signal(barrier, inc=1, device_id={"ep": other}, device_id_type=MESH)

        return carry

    lax.fori_loop(0, n_ep, greet, 0)
    pl.semaphore_signal(barrier, inc=1, device_id={"tp": right}, device_id_type=MESH)
    pl.semaphore_signal(barrier, inc=1, device_id={"tp": left}, device_id_type=MESH)

    for n in range(gate_tiles):
        for part, ref in enumerate((gate_ref, up_ref)):
            pltpu.make_async_copy(
                ref.at[0, :, pl.ds(128 * n, 128)], wgu.at[n, :, pl.ds(128 * part, 128)], w_sem.at[0]
            ).start()
    for n in range(down_tiles):
        pltpu.make_async_copy(
            down_ref.at[0, :, pl.ds(256 * n, 256)], wdn.at[n], w_sem.at[1]
        ).start()

    pltpu.make_async_copy(project_ref, wproj, w_sem.at[2]).start()

    for n, (src, dst) in enumerate(inputs):
        pltpu.make_async_copy(src, dst, i_sem.at[n]).wait()

    tok = tokens_ref.shape[0]
    e_rows = [routes_ref[0:1, :], routes_ref[1:2, :]]
    expert_id = lax.broadcasted_iota(jnp.int32, (N_Z * N_YC, tok), 0)
    named = [jnp.where(expert_id == e, 1.0, 0.0) for e in e_rows]
    before = jnp.where(
        lax.broadcasted_iota(jnp.int32, (tok, tok), 0)
        < lax.broadcasted_iota(jnp.int32, (tok, tok), 1),
        1.0,
        0.0,
    ).astype(jnp.bfloat16)
    ranks = [
        jnp.dot(n.astype(jnp.bfloat16), before, preferred_element_type=jnp.float32) for n in named
    ]
    ranks[1] = ranks[1] + jnp.sum(named[0], axis=1, keepdims=True)
    slots = []
    flat_offsets = [o for pair in OFFSETS for o in pair]
    for e, n, r in zip(e_rows, named, ranks):
        rank = jnp.sum(n * r, axis=0, keepdims=True).astype(jnp.int32)
        offset = (lax.shift_right_logical(e, 3) - z) & (N_Z - 1)
        place = jnp.zeros_like(offset)
        for p, o in enumerate(flat_offsets):
            place = jnp.where(offset == o, p, place)
        slots.append((place * N_YC + (e & (N_YC - 1))) * CAP + rank)

    i256 = lax.broadcasted_iota(jnp.int32, (256, 256), 0)
    j256 = lax.broadcasted_iota(jnp.int32, (256, 256), 1)
    perm_ref[...] = jnp.where(
        j256 == (i256 & 15) * 16 + lax.shift_right_logical(i256, 4), 1.0, 0.0
    ).astype(jnp.bfloat16)

    x = tokens_ref[...].astype(jnp.float32)
    squares = jnp.mean(x * x, axis=-1, keepdims=True)
    row_ref[...] = (x * lax.rsqrt(squares + norm_eps) * gain_ref[...]).astype(jnp.bfloat16)

    def peer(i, y, sign, k):
        return lax.rem(z + (sign * OFFSETS[k][i]) % N_Z, jnp.int32(N_Z)) * N_YC + y

    def a_copy(k, i, y):
        return pltpu.make_async_remote_copy(
            src_ref=outb.at[k, i * N_YC + y],
            dst_ref=recv.at[k, i * N_YC + yc],
            send_sem=a_send.at[k],
            recv_sem=a_recv.at[k],
            device_id={"ep": peer(i, y, 1, k)},
            device_id_type=MESH,
        )

    def b_copy(k, i, y):
        return pltpu.make_async_remote_copy(
            src_ref=back.at[k, i * N_YC + y],
            dst_ref=ret.at[k, i * N_YC + yc],
            send_sem=b_send.at[k],
            recv_sem=b_recv.at[k],
            device_id={"ep": peer(i, y, -1, k)},
            device_id_type=MESH,
        )

    def spread(copy_of, k):
        def one(j, carry):
            y = (yc + 1 + j) & (N_YC - 1)
            for i in range(HALVES):
                if OFFSETS[k][i] == 0:

                    @pl.when(y != yc)
                    def _():
                        copy_of(k, i, y).start()
                else:
                    copy_of(k, i, y).start()
            return carry

        lax.fori_loop(0, N_YC, one, 0)

    def bulk(buffer, sem, k):
        count = HALVES * N_YC - (k == SELF_CHUNK)
        view = buffer.at[k, pl.ds(0, count)]
        pltpu.make_async_copy(view, view, sem.at[k]).wait()

    def dispatch(k):
        row_id = lax.broadcasted_iota(jnp.int32, (ROWS, tok), 0) + k * ROWS
        hits = [row_id == s for s in slots]
        select = jnp.where(jnp.logical_or(hits[0], hits[1]), 1.0, 0.0).astype(jnp.bfloat16)
        shares = jnp.where(hits[0], weights_ref[0:1, :], 0.0) + jnp.where(
            hits[1], weights_ref[1:2, :], 0.0
        )
        coarse = shares.astype(jnp.bfloat16)
        mix[k, 0] = coarse
        mix[k, 1] = (shares - coarse.astype(jnp.float32)).astype(jnp.bfloat16)
        block = jnp.dot(select, row_ref[...], preferred_element_type=jnp.float32)
        tiles = rows_to_tiles(block.astype(jnp.bfloat16), perm_ref[...], width)
        flat = outb.at[k].reshape(ROWS, 16, lanes)
        for g in range(GROUPS):
            flat[16 * g : 16 * g + 16] = tiles[g]
        if k == SELF_CHUNK:
            recv[k, yc] = outb[k, yc]

    follower = lax.rem(me + 1, jnp.int32(N_Z * N_YC))

    def h_copy(which):
        ref = (keys_ref, values_ref)[which]
        return pltpu.make_async_remote_copy(
            src_ref=ref.at[:, pl.ds(ref.shape[1] - WINDOW, WINDOW)],
            dst_ref=halo.at[which],
            send_sem=h_send.at[which],
            recv_sem=h_recv.at[which],
            device_id={"ep": follower},
            device_id_type=MESH,
        )

    def begin():
        pl.semaphore_wait(barrier, n_ep - 1 + 2)
        h_copy(0).start()
        h_copy(1).start()

    def send(k):
        spread(a_copy, k)

    heads = queries_ref.shape[0] // HDIM
    sinks = jnp.concatenate(
        [jnp.broadcast_to(sink_ref[0:1, h : h + 1], (1, WINDOW)) for h in range(heads)], axis=1
    )
    key_i = lax.broadcasted_iota(jnp.int32, (2 * WINDOW, heads * WINDOW), 0)
    query_i = lax.broadcasted_iota(jnp.int32, (2 * WINDOW, heads * WINDOW), 1) & (WINDOW - 1)
    in_window = jnp.logical_and(key_i > query_i, key_i <= query_i + WINDOW)

    def attend(b, keys, values, allowed):
        at = slice(WINDOW * b, WINDOW * b + WINDOW)
        block = jnp.concatenate(
            [queries_ref[HDIM * h : HDIM * h + HDIM, at] for h in range(heads)], axis=1
        )
        scores = lax.dot_general(
            keys, block, (((0,), (0,)), ((), ())), preferred_element_type=jnp.float32
        ) * HDIM ** (-0.5)
        logits = jnp.where(allowed, scores, masked_value)
        top = jnp.maximum(jnp.max(logits, axis=0, keepdims=True), sinks)
        exponent = jnp.exp(logits - top)
        denominator = jnp.sum(exponent, axis=0, keepdims=True) + jnp.exp(sinks - top)
        probs = (exponent / denominator).astype(jnp.bfloat16)
        result = jnp.dot(values, probs, preferred_element_type=jnp.float32).astype(jnp.bfloat16)
        for h in range(heads):
            attended[HDIM * h : HDIM * h + HDIM, at] = result[:, WINDOW * h : WINDOW * h + WINDOW]

    blocks = queries_ref.shape[1] // WINDOW
    own_rows = mpart.shape[1]
    block_parts = WINDOW // own_rows

    def project(b):
        at_rows = slice(WINDOW * b, WINDOW * b + WINDOW)
        for n in range(width // 512):
            at = slice(512 * n, 512 * n + 512)
            part = lax.dot_general(
                attended[:, at_rows],
                wproj[:, at],
                (((0,), (0,)), ((), ())),
                preferred_element_type=jnp.float32,
            ).astype(jnp.bfloat16)
            mpart[block_parts * b : block_parts * b + block_parts, :, at] = part.reshape(
                block_parts, own_rows, 512
            )

    def mixer_own():
        for b in range(1, blocks):
            at = slice(WINDOW * (b - 1), WINDOW * (b + 1))
            attend(b, keys_ref[:, at], values_ref[:, at], in_window)
        pltpu.make_async_copy(wproj, wproj, w_sem.at[2]).wait()
        for b in range(1, blocks):
            project(b)

    def mixer_halo():
        with jax.named_scope("halo_wait"):
            h_copy(0).wait_recv()
            h_copy(1).wait_recv()
        first = slice(0, WINDOW)
        attend(
            0,
            jnp.concatenate([halo[0], keys_ref[:, first]], axis=1),
            jnp.concatenate([halo[1], values_ref[:, first]], axis=1),
            jnp.logical_and(in_window, jnp.logical_or(key_i >= WINDOW, me > 0)),
        )
        project(0)

    across = lax.rem(tp + 2, jnp.int32(n_tp))
    left_half = pl.ds(0, half)
    right_half = pl.ds(half, half)

    def m_copy(which):
        if which == 0:
            src, dst, to = mpart.at[across, :, left_half], m1.at[0], right
        elif which == 1:
            src, dst, to = mpart.at[across, :, right_half], m1.at[1], left
        elif which == 2:
            src, dst, to = mpart.at[right, :, right_half], m2.at[0, :, right_half], right
        elif which == 3:
            src, dst, to = mpart.at[left, :, left_half], m2.at[1, :, left_half], left
        elif which == 4:
            src, dst, to = mpart.at[right, :, left_half], m2.at[0, :, left_half], right
        else:
            src, dst, to = mpart.at[left, :, right_half], m2.at[1, :, right_half], left
        return pltpu.make_async_remote_copy(
            src_ref=src,
            dst_ref=dst,
            send_sem=m_send.at[which],
            recv_sem=m_recv.at[which],
            device_id={"tp": to},
            device_id_type=MESH,
        )

    def mixer_transit():
        m_copy(0).start()
        m_copy(1).start()

    def mixer_direct():
        m_copy(2).start()
        m_copy(3).start()

    def mixer_relay():
        m_copy(0).wait_recv()
        mpart[right, :, left_half] = (
            mpart[right, :, left_half].astype(jnp.float32) + m1[0].astype(jnp.float32)
        ).astype(jnp.bfloat16)
        m_copy(4).start()
        m_copy(1).wait_recv()
        mpart[left, :, right_half] = (
            mpart[left, :, right_half].astype(jnp.float32) + m1[1].astype(jnp.float32)
        ).astype(jnp.bfloat16)
        m_copy(5).start()

    def mixer_finish():
        for which in range(2, 6):
            m_copy(which).wait_recv()
        total = (
            mpart[tp].astype(jnp.float32)
            + m2[0].astype(jnp.float32)
            + m2[1].astype(jnp.float32)
        )
        squares = jnp.mean(total * total, axis=-1, keepdims=True)
        mixed_ref[...] = (total * lax.rsqrt(squares + norm_eps) * mix_gain_ref[...]).astype(
            jnp.bfloat16
        )
        pltpu.make_async_copy(mixed_ref, mixed_out, o_sem.at[0]).start()

    low = pl.ds(0, half)
    high = pl.ds(half, half)

    def g_copy(k, which):
        if which == 0:
            src, dst, to = xbuf.at[k, 0], xbuf.at[k, 1], right
        elif which == 1:
            src, dst, to = xbuf.at[k, 0], xbuf.at[k, 2], left
        elif which == 2:
            src, dst, to = xbuf.at[k, 1, :, low], xbuf.at[k, 3, :, low], right
        else:
            src, dst, to = xbuf.at[k, 2, :, high], xbuf.at[k, 3, :, high], left
        return pltpu.make_async_remote_copy(
            src_ref=src,
            dst_ref=dst,
            send_sem=g_send.at[k, which],
            recv_sem=g_recv.at[k, which],
            device_id={"tp": to},
            device_id_type=MESH,
        )

    def q_copy(k, which):
        if which == 0:
            src, dst, to = pbuf.at[k, 3, :, low], r1.at[k, 0], right
        elif which == 1:
            src, dst, to = pbuf.at[k, 3, :, high], r1.at[k, 1], left
        elif which == 2:
            src, dst, to = pbuf.at[k, 2, :, high], r2.at[k, 0, :, high], right
        elif which == 3:
            src, dst, to = pbuf.at[k, 1, :, low], r2.at[k, 1, :, low], left
        elif which == 4:
            src, dst, to = pbuf.at[k, 2, :, low], r2.at[k, 0, :, low], right
        else:
            src, dst, to = pbuf.at[k, 1, :, high], r2.at[k, 1, :, high], left
        return pltpu.make_async_remote_copy(
            src_ref=src,
            dst_ref=dst,
            send_sem=q_send.at[k, which],
            recv_sem=q_recv.at[k, which],
            device_id={"tp": to},
            device_id_type=MESH,
        )

    def arrive(k):
        with jax.named_scope("arrive_wait"):
            bulk(recv, a_recv, k)
        rows = tiles_to_rows(recv[k].reshape(ROWS, 16, lanes), perm_ref[...], lanes)
        for g in range(GROUPS):
            for s in range(16):
                xbuf[k, 0, 16 * g : 16 * g + 16, lanes * s : lanes * s + lanes] = rows[g][s]
        g_copy(k, 0).start()
        g_copy(k, 1).start()

    def forward(k):
        with jax.named_scope("forward_wait"):
            g_copy(k, 0).wait_recv()
            g_copy(k, 2).start()
            g_copy(k, 1).wait_recv()
            g_copy(k, 3).start()

    def multiply(k, sends=True):
        if k == first_multiplied:
            pltpu.make_async_copy(wgu, wgu, w_sem.at[0]).wait()
            pltpu.make_async_copy(wdn, wdn, w_sem.at[1]).wait()

        with jax.named_scope("multiply_wait"):
            g_copy(k, 2).wait_recv()
            g_copy(k, 3).wait_recv()
        for n in range(gate_tiles):
            both = jnp.dot(
                xbuf[k].reshape(n_tp * ROWS, width), wgu[n], preferred_element_type=jnp.float32
            )
            gate, up = both[:, :128], both[:, 128:]
            hid[:, 128 * n : 128 * n + 128] = (gate / (1.0 + jnp.exp(-gate)) * up).astype(
                jnp.bfloat16
            )
        for n in range(down_tiles):
            part = jnp.dot(hid[...], wdn[n], preferred_element_type=jnp.float32)
            pbuf[k, :, :, 256 * n : 256 * n + 256] = part.astype(jnp.bfloat16).reshape(
                n_tp, ROWS, 256
            )
            if sends and n == down_tiles // 2 - 1:
                q_copy(k, 0).start()
        if sends:
            for which in range(1, 4):
                q_copy(k, which).start()

    def hand_on(k):
        for which in range(4):
            q_copy(k, which).start()

    def relay(k):
        with jax.named_scope("relay_wait"):
            q_copy(k, 0).wait_recv()
        pbuf[k, 2, :, low] = (
            pbuf[k, 2, :, low].astype(jnp.float32) + r1[k, 0].astype(jnp.float32)
        ).astype(jnp.bfloat16)
        q_copy(k, 4).start()
        q_copy(k, 1).wait_recv()
        pbuf[k, 1, :, high] = (
            pbuf[k, 1, :, high].astype(jnp.float32) + r1[k, 1].astype(jnp.float32)
        ).astype(jnp.bfloat16)
        q_copy(k, 5).start()

    def finish(k):
        with jax.named_scope("finish_wait"):
            for which in range(2, 6):
                q_copy(k, which).wait_recv()
        total = (
            pbuf[k, 0].astype(jnp.float32)
            + r2[k, 0].astype(jnp.float32)
            + r2[k, 1].astype(jnp.float32)
        ).astype(jnp.bfloat16)
        tiles = rows_to_tiles(total, perm_ref[...], width)
        flat = back.at[k].reshape(ROWS, 16, lanes)
        for g in range(GROUPS):
            flat[16 * g : 16 * g + 16] = tiles[g]
        if k == SELF_CHUNK:
            ret[k, yc] = back[k, yc]

        spread(b_copy, k)

    def combine(k):
        with jax.named_scope("combine_wait"):
            bulk(ret, b_recv, k)
        rows = tiles_to_rows(ret[k].reshape(ROWS, 16, lanes), perm_ref[...], lanes)
        block = jnp.concatenate([jnp.concatenate(r, axis=1) for r in rows], axis=0)
        dims = (((0,), (0,)), ((), ()))
        part = lax.dot_general(
            mix[k, 0], block, dims, preferred_element_type=jnp.float32
        ) + lax.dot_general(mix[k, 1], block, dims, preferred_element_type=jnp.float32)
        if k == last_combined:
            out_ref[...] = (acc[...] + part).astype(jnp.bfloat16)
            pltpu.make_async_copy(out_ref, moe_out, o_sem.at[1]).start()
        elif k == first_combined:
            acc[...] = part
        else:
            acc[...] += part

    stages = dict(
        D=dispatch,
        B=begin,
        S=send,
        O=mixer_own,
        H=mixer_halo,
        P=mixer_transit,
        Q=mixer_direct,
        R=mixer_relay,
        X=mixer_finish,
        A=arrive,
        F=forward,
        W=multiply,
        M=functools.partial(multiply, sends=False),
        T=hand_on,
        L=relay,
        E=finish,
        C=combine,
    )
    order = ORDER.split()
    first_multiplied = [int(o[1]) for o in order if o[0] in "MW"][0]
    combined = [int(o[1]) for o in order if o[0] == "C"]
    first_combined, last_combined = combined[0], combined[-1]
    for op in order:
        with jax.named_scope(op):
            stages[op[0]](*(int(k) for k in op[1:]))

    def drain(k):
        bulk(outb, a_send, k)
        bulk(back, b_send, k)
        for which in range(4):
            g_copy(k, which).wait_send()
        for which in range(6):
            q_copy(k, which).wait_send()

    with jax.named_scope("drain"):
        pltpu.make_async_copy(mixed_ref, mixed_out, o_sem.at[0]).wait()
        pltpu.make_async_copy(out_ref, moe_out, o_sem.at[1]).wait()
        for which in range(2):
            h_copy(which).wait_send()
        for which in range(6):
            m_copy(which).wait_send()
        for k in range(CHUNKS):
            drain(k)


def settle_kernel(mixed_in, moe_in, mixed_out, moe_out, mixed_ref, moe_ref, in_sem, out_sem):
    pieces = [(mixed_in, mixed_ref, mixed_out, 0)] + [
        (moe_in, moe_ref, moe_out, SETTLE_ROWS * p) for p in range(moe_ref.shape[0] // SETTLE_ROWS)
    ]
    loads, stores = [], []
    for n, (src, held, dst, first) in enumerate(pieces):
        rows = pl.ds(first, SETTLE_ROWS)
        loads.append(pltpu.make_async_copy(src.at[rows], held.at[rows], in_sem.at[n]))
        stores.append(pltpu.make_async_copy(held.at[rows], dst.at[rows], out_sem.at[n]))
    for load in loads:
        load.start()
    for load, store in zip(loads, stores):
        load.wait()
        store.start()
    for store in stores:
        store.wait()


def settle(mixed, moe):
    pieces = 1 + moe.shape[0] // SETTLE_ROWS
    hbm = pl.BlockSpec(memory_space=pl.ANY)
    return pl.pallas_call(
        settle_kernel,
        out_shape=tuple(jax.ShapeDtypeStruct(a.shape, a.dtype) for a in (mixed, moe)),
        in_specs=[hbm, hbm],
        out_specs=(hbm, hbm),
        scratch_shapes=[
            pltpu.VMEM(mixed.shape, mixed.dtype),
            pltpu.VMEM(moe.shape, moe.dtype),
            pltpu.SemaphoreType.DMA((pieces,)),
            pltpu.SemaphoreType.DMA((pieces,)),
        ],
        compiler_params=pltpu.CompilerParams(vmem_limit_bytes=58 * 1024 * 1024),
    )(mixed, moe)


def shards(
    queries,
    key_rows,
    value_rows,
    sink_logits,
    out_weight,
    mix_gain,
    moe_tokens,
    moe_gain,
    routes,
    route_weights,
    expert_gate,
    expert_up,
    expert_down,
):
    tok, width = moe_tokens.shape
    n_tp = lax.axis_size("tp")
    hidden = expert_gate.shape[2]
    lanes = width // 16
    own_rows = queries.shape[0] // n_tp
    bf16 = jnp.bfloat16
    hbm = pl.BlockSpec(memory_space=pl.ANY)
    dma = pltpu.SemaphoreType.DMA
    tiles = (CHUNKS, HALVES * N_YC, CAP, 16, lanes)
    small = (
        moe_tokens,
        moe_gain[None, :],
        routes.T,
        route_weights.T,
        queries.T,
        key_rows.T,
        value_rows.T,
        sink_logits[None, :],
        mix_gain[None, :],
    )
    mixed, moe = pl.pallas_call(
        functools.partial(layer_kernel, n_tp),
        out_shape=(
            jax.ShapeDtypeStruct((own_rows, width), bf16),
            jax.ShapeDtypeStruct((tok, width), bf16),
        ),
        in_specs=[hbm] * 13,
        out_specs=(hbm, hbm),
        scratch_shapes=[
            *[pltpu.VMEM(a.shape, a.dtype) for a in small],
            pltpu.VMEM((own_rows, width), bf16),
            pltpu.VMEM((tok, width), bf16),
            pltpu.VMEM(tiles, bf16),
            pltpu.VMEM(tiles, bf16),
            pltpu.VMEM((CHUNKS, n_tp, ROWS, width), bf16),
            pltpu.VMEM((CHUNKS, n_tp, ROWS, width), bf16),
            pltpu.VMEM((CHUNKS, 2, ROWS, width // 2), bf16),
            pltpu.VMEM((CHUNKS, 2, ROWS, width), bf16),
            pltpu.VMEM(tiles, bf16),
            pltpu.VMEM(tiles, bf16),
            pltpu.VMEM((hidden // 128, width, 256), bf16),
            pltpu.VMEM((width // 256, hidden, 256), bf16),
            pltpu.VMEM((n_tp * ROWS, hidden), bf16),
            pltpu.VMEM((tok, width), jnp.float32),
            pltpu.VMEM((CHUNKS, 2, ROWS, tok), bf16),
            pltpu.VMEM((256, 256), bf16),
            pltpu.VMEM((tok, width), bf16),
            pltpu.VMEM((2, HDIM, WINDOW), bf16),
            pltpu.VMEM((queries.shape[1], queries.shape[0]), bf16),
            pltpu.VMEM(out_weight.shape, bf16),
            pltpu.VMEM((n_tp, own_rows, width), bf16),
            pltpu.VMEM((2, own_rows, width // 2), bf16),
            pltpu.VMEM((2, own_rows, width), bf16),
            dma((len(small),)),
            dma((2,)),
            dma((2,)),
            dma((2,)),
            dma((6,)),
            dma((6,)),
            dma((3,)),
            dma((CHUNKS,)),
            dma((CHUNKS,)),
            dma((CHUNKS, 4)),
            dma((CHUNKS, 4)),
            dma((CHUNKS, 6)),
            dma((CHUNKS, 6)),
            dma((CHUNKS,)),
            dma((CHUNKS,)),
        ],
        compiler_params=pltpu.CompilerParams(
            collective_id=0, has_side_effects=True, vmem_limit_bytes=58 * 1024 * 1024
        ),
    )(*small, expert_gate, expert_up, expert_down, out_weight)
    return settle(mixed, moe)


def solution(mesh):
    return jax.shard_map(
        shards,
        mesh=mesh,
        in_specs=(
            P("ep", "tp"),
            P("ep", "tp"),
            P("ep", "tp"),
            P("tp"),
            P("tp", None),
            P(),
            P(("ep", "tp"), None),
            P(),
            P(("ep", "tp"), None),
            P(("ep", "tp"), None),
            P("ep", None, "tp"),
            P("ep", None, "tp"),
            P("ep", "tp", None),
        ),
        out_specs=(P(("ep", "tp"), None), P(("ep", "tp"), None)),
        check_vma=False,
    )
```

```python
import functools

import jax
import jax.numpy as jnp
from jax import lax
from jax.experimental import pallas as pl
from jax.experimental.pallas import tpu as pltpu
from jax.sharding import PartitionSpec as P

HDIM = 64
WINDOW = 128
MESH = pl.DeviceIdType.MESH

norm_eps = 1e-06
masked_value = -1e30

N_Z = 8
N_YC = 8
CAP = 5
CHUNKS = 4
HALVES = 2
OFFSETS = ((2, 6), (4, 7), (3, 5), (0, 1))
SELF_CHUNK = 3
ORDER = (
    "D3", "B", "S3", "D0", "S0", "O", "D1", "D2", "H", "Q", "A3", "S1", "A0", "F3", "S2", "A1",
    "F0", "M3", "F1", "A2", "W1", "M0", "F2", "L1", "T0", "M2", "E1", "L0", "T2", "E0", "L2", "T3",
    "C1", "E2", "L3", "P", "C0", "E3", "R", "C2", "X", "C3",
)
ROWS = HALVES * N_YC * CAP
GROUPS = ROWS // 16


def rows_to_tiles(block, perm, width):
    lanes = width // 16
    stacked = jnp.concatenate(
        [
            jnp.concatenate(
                [block[16 * g : 16 * g + 16, lanes * s : lanes * s + lanes] for s in range(16)],
                axis=0,
            )
            for g in range(GROUPS)
        ],
        axis=1,
    )
    turned = jnp.dot(perm, stacked, preferred_element_type=jnp.float32).astype(jnp.bfloat16)
    return [turned[:, lanes * g : lanes * g + lanes].reshape(16, 16, lanes) for g in range(GROUPS)]


def tiles_to_rows(tiles, perm, lanes):
    stacked = jnp.concatenate(
        [tiles[16 * g : 16 * g + 16].reshape(256, lanes) for g in range(GROUPS)], axis=1
    )
    turned = jnp.dot(perm, stacked, preferred_element_type=jnp.float32).astype(jnp.bfloat16)
    return [
        [turned[16 * s : 16 * s + 16, lanes * g : lanes * g + lanes] for s in range(16)]
        for g in range(GROUPS)
    ]


def layer_kernel(
    n_tp,
    tokens_in,
    gain_in,
    routes_in,
    weights_in,
    queries_in,
    keys_in,
    values_in,
    sink_in,
    mix_gain_in,
    gate_ref,
    up_ref,
    down_ref,
    project_ref,
    mixed_ref,
    out_ref,
    tokens_ref,
    gain_ref,
    routes_ref,
    weights_ref,
    queries_ref,
    keys_ref,
    values_ref,
    sink_ref,
    mix_gain_ref,
    outb,
    recv,
    xbuf,
    pbuf,
    r1,
    r2,
    back,
    ret,
    wgu,
    wdn,
    hid,
    acc,
    mix,
    perm_ref,
    row_ref,
    halo,
    attended,
    wproj,
    mpart,
    m1,
    m2,
    i_sem,
    h_send,
    h_recv,
    m_send,
    m_recv,
    w_sem,
    a_send,
    a_recv,
    g_send,
    g_recv,
    q_send,
    q_recv,
    b_send,
    b_recv,
):
    width = tokens_ref.shape[1]
    half = width // 2
    lanes = width // 16
    gate_tiles = wgu.shape[0]
    down_tiles = wdn.shape[0]
    me = lax.axis_index("ep")
    tp = lax.axis_index("tp")
    z = lax.div(me, jnp.int32(N_YC))
    yc = lax.rem(me, jnp.int32(N_YC))
    right = lax.rem(tp + 1, jnp.int32(n_tp))
    left = lax.rem(tp + n_tp - 1, jnp.int32(n_tp))

    inputs = (
        (routes_in, routes_ref),
        (tokens_in, tokens_ref),
        (gain_in, gain_ref),
        (weights_in, weights_ref),
        (keys_in, keys_ref),
        (values_in, values_ref),
        (queries_in, queries_ref),
        (sink_in, sink_ref),
        (mix_gain_in, mix_gain_ref),
    )
    for n, (src, dst) in enumerate(inputs):
        pltpu.make_async_copy(src, dst, i_sem.at[n]).start()

    barrier = pltpu.get_barrier_semaphore()

    n_ep = N_Z * N_YC

    def greet(i, carry):
        ahead = lax.rem(me + n_ep // 2 + i, jnp.int32(n_ep))
        behind = lax.rem(me + n_ep // 2 - 1 - i + n_ep, jnp.int32(n_ep))
        pl.semaphore_signal(barrier, inc=1, device_id={"ep": ahead}, device_id_type=MESH)

        @pl.when(behind != me)
        def _():
            pl.semaphore_signal(barrier, inc=1, device_id={"ep": behind}, device_id_type=MESH)

        return carry

    lax.fori_loop(0, n_ep // 2, greet, 0)
    pl.semaphore_signal(barrier, inc=1, device_id={"tp": right}, device_id_type=MESH)
    pl.semaphore_signal(barrier, inc=1, device_id={"tp": left}, device_id_type=MESH)

    for n in range(gate_tiles):
        for part, ref in enumerate((gate_ref, up_ref)):
            pltpu.make_async_copy(
                ref.at[0, :, pl.ds(128 * n, 128)], wgu.at[n, :, pl.ds(128 * part, 128)], w_sem.at[0]
            ).start()
    for n in range(down_tiles):
        pltpu.make_async_copy(
            down_ref.at[0, :, pl.ds(256 * n, 256)], wdn.at[n], w_sem.at[1]
        ).start()

    pltpu.make_async_copy(project_ref, wproj, w_sem.at[2]).start()

    for n, (src, dst) in enumerate(inputs):
        pltpu.make_async_copy(src, dst, i_sem.at[n]).wait()

    tok = tokens_ref.shape[0]
    e_rows = [routes_ref[0:1, :], routes_ref[1:2, :]]
    expert_id = lax.broadcasted_iota(jnp.int32, (N_Z * N_YC, tok), 0)
    named = [jnp.where(expert_id == e, 1.0, 0.0) for e in e_rows]
    before = jnp.where(
        lax.broadcasted_iota(jnp.int32, (tok, tok), 0)
        < lax.broadcasted_iota(jnp.int32, (tok, tok), 1),
        1.0,
        0.0,
    ).astype(jnp.bfloat16)
    ranks = [
        jnp.dot(n.astype(jnp.bfloat16), before, preferred_element_type=jnp.float32) for n in named
    ]
    ranks[1] = ranks[1] + jnp.sum(named[0], axis=1, keepdims=True)
    slots = []
    flat_offsets = [o for pair in OFFSETS for o in pair]
    for e, n, r in zip(e_rows, named, ranks):
        rank = jnp.sum(n * r, axis=0, keepdims=True).astype(jnp.int32)
        offset = (lax.shift_right_logical(e, 3) - z) & (N_Z - 1)
        place = jnp.zeros_like(offset)
        for p, o in enumerate(flat_offsets):
            place = jnp.where(offset == o, p, place)
        slots.append((place * N_YC + (e & (N_YC - 1))) * CAP + rank)

    i256 = lax.broadcasted_iota(jnp.int32, (256, 256), 0)
    j256 = lax.broadcasted_iota(jnp.int32, (256, 256), 1)
    perm_ref[...] = jnp.where(
        j256 == (i256 & 15) * 16 + lax.shift_right_logical(i256, 4), 1.0, 0.0
    ).astype(jnp.bfloat16)

    x = tokens_ref[...].astype(jnp.float32)
    squares = jnp.mean(x * x, axis=-1, keepdims=True)
    row_ref[...] = (x * lax.rsqrt(squares + norm_eps) * gain_ref[...]).astype(jnp.bfloat16)

    def peer(i, y, sign, k):
        return lax.rem(z + (sign * OFFSETS[k][i]) % N_Z, jnp.int32(N_Z)) * N_YC + y

    def a_copy(k, i, y):
        return pltpu.make_async_remote_copy(
            src_ref=outb.at[k, i * N_YC + y],
            dst_ref=recv.at[k, i * N_YC + yc],
            send_sem=a_send.at[k],
            recv_sem=a_recv.at[k],
            device_id={"ep": peer(i, y, 1, k)},
            device_id_type=MESH,
        )

    def b_copy(k, i, y):
        return pltpu.make_async_remote_copy(
            src_ref=back.at[k, i * N_YC + y],
            dst_ref=ret.at[k, i * N_YC + yc],
            send_sem=b_send.at[k],
            recv_sem=b_recv.at[k],
            device_id={"ep": peer(i, y, -1, k)},
            device_id_type=MESH,
        )

    def spread(copy_of, k):
        def one(j, carry, halves):
            y = (yc + N_YC // 2 + j) & (N_YC - 1)
            for i in halves:
                if OFFSETS[k][i] == 0:

                    @pl.when(y != yc)
                    def _():
                        copy_of(k, i, y).start()
                else:
                    copy_of(k, i, y).start()
            return carry

        for halves in ((1,), (0,)) if k == SELF_CHUNK else ((0, 1),):
            lax.fori_loop(0, N_YC, functools.partial(one, halves=halves), 0)

    def bulk(buffer, sem, k):
        count = HALVES * N_YC - (k == SELF_CHUNK)
        view = buffer.at[k, pl.ds(0, count)]
        pltpu.make_async_copy(view, view, sem.at[k]).wait()

    def dispatch(k):
        row_id = lax.broadcasted_iota(jnp.int32, (ROWS, tok), 0) + k * ROWS
        hits = [row_id == s for s in slots]
        select = jnp.where(jnp.logical_or(hits[0], hits[1]), 1.0, 0.0).astype(jnp.bfloat16)
        shares = jnp.where(hits[0], weights_ref[0:1, :], 0.0) + jnp.where(
            hits[1], weights_ref[1:2, :], 0.0
        )
        coarse = shares.astype(jnp.bfloat16)
        mix[k, 0] = coarse
        mix[k, 1] = (shares - coarse.astype(jnp.float32)).astype(jnp.bfloat16)
        block = jnp.dot(select, row_ref[...], preferred_element_type=jnp.float32)
        tiles = rows_to_tiles(block.astype(jnp.bfloat16), perm_ref[...], width)
        flat = outb.at[k].reshape(ROWS, 16, lanes)
        for g in range(GROUPS):
            flat[16 * g : 16 * g + 16] = tiles[g]
        if k == SELF_CHUNK:
            recv[k, yc] = outb[k, yc]

    follower = lax.rem(me + 1, jnp.int32(N_Z * N_YC))

    def h_copy(which):
        ref = (keys_ref, values_ref)[which]
        return pltpu.make_async_remote_copy(
            src_ref=ref.at[:, pl.ds(ref.shape[1] - WINDOW, WINDOW)],
            dst_ref=halo.at[which],
            send_sem=h_send.at[which],
            recv_sem=h_recv.at[which],
            device_id={"ep": follower},
            device_id_type=MESH,
        )

    def begin():
        pl.semaphore_wait(barrier, n_ep - 1 + 2)
        h_copy(0).start()
        h_copy(1).start()

    def send(k):
        spread(a_copy, k)

    heads = queries_ref.shape[0] // HDIM
    sinks = jnp.concatenate(
        [jnp.broadcast_to(sink_ref[0:1, h : h + 1], (1, WINDOW)) for h in range(heads)], axis=1
    )
    key_i = lax.broadcasted_iota(jnp.int32, (2 * WINDOW, heads * WINDOW), 0)
    query_i = lax.broadcasted_iota(jnp.int32, (2 * WINDOW, heads * WINDOW), 1) & (WINDOW - 1)
    in_window = jnp.logical_and(key_i > query_i, key_i <= query_i + WINDOW)

    def attend(b, keys, values, allowed):
        at = slice(WINDOW * b, WINDOW * b + WINDOW)
        block = jnp.concatenate(
            [queries_ref[HDIM * h : HDIM * h + HDIM, at] for h in range(heads)], axis=1
        )
        scores = lax.dot_general(
            keys, block, (((0,), (0,)), ((), ())), preferred_element_type=jnp.float32
        ) * HDIM ** (-0.5)
        logits = jnp.where(allowed, scores, masked_value)
        top = jnp.maximum(jnp.max(logits, axis=0, keepdims=True), sinks)
        exponent = jnp.exp(logits - top)
        denominator = jnp.sum(exponent, axis=0, keepdims=True) + jnp.exp(sinks - top)
        probs = (exponent / denominator).astype(jnp.bfloat16)
        result = jnp.dot(values, probs, preferred_element_type=jnp.float32).astype(jnp.bfloat16)
        for h in range(heads):
            attended[HDIM * h : HDIM * h + HDIM, at] = result[:, WINDOW * h : WINDOW * h + WINDOW]

    blocks = queries_ref.shape[1] // WINDOW
    own_rows = mpart.shape[1]
    block_parts = WINDOW // own_rows

    def project(b):
        at_rows = slice(WINDOW * b, WINDOW * b + WINDOW)
        for n in range(width // 512):
            at = slice(512 * n, 512 * n + 512)
            part = lax.dot_general(
                attended[:, at_rows],
                wproj[:, at],
                (((0,), (0,)), ((), ())),
                preferred_element_type=jnp.float32,
            ).astype(jnp.bfloat16)
            mpart[block_parts * b : block_parts * b + block_parts, :, at] = part.reshape(
                block_parts, own_rows, 512
            )

    def mixer_own():
        for b in range(1, blocks):
            at = slice(WINDOW * (b - 1), WINDOW * (b + 1))
            attend(b, keys_ref[:, at], values_ref[:, at], in_window)
        pltpu.make_async_copy(wproj, wproj, w_sem.at[2]).wait()
        for b in range(1, blocks):
            project(b)

    def mixer_halo():
        with jax.named_scope("halo_wait"):
            h_copy(0).wait_recv()
            h_copy(1).wait_recv()
        first = slice(0, WINDOW)
        attend(
            0,
            jnp.concatenate([halo[0], keys_ref[:, first]], axis=1),
            jnp.concatenate([halo[1], values_ref[:, first]], axis=1),
            jnp.logical_and(in_window, jnp.logical_or(key_i >= WINDOW, me > 0)),
        )
        project(0)

    across = lax.rem(tp + 2, jnp.int32(n_tp))
    left_half = pl.ds(0, half)
    right_half = pl.ds(half, half)

    def m_copy(which):
        if which == 0:
            src, dst, to = mpart.at[across, :, left_half], m1.at[0], right
        elif which == 1:
            src, dst, to = mpart.at[across, :, right_half], m1.at[1], left
        elif which == 2:
            src, dst, to = mpart.at[right, :, right_half], m2.at[0, :, right_half], right
        elif which == 3:
            src, dst, to = mpart.at[left, :, left_half], m2.at[1, :, left_half], left
        elif which == 4:
            src, dst, to = mpart.at[right, :, left_half], m2.at[0, :, left_half], right
        else:
            src, dst, to = mpart.at[left, :, right_half], m2.at[1, :, right_half], left
        return pltpu.make_async_remote_copy(
            src_ref=src,
            dst_ref=dst,
            send_sem=m_send.at[which],
            recv_sem=m_recv.at[which],
            device_id={"tp": to},
            device_id_type=MESH,
        )

    def mixer_transit():
        m_copy(0).start()
        m_copy(1).start()

    def mixer_direct():
        m_copy(2).start()
        m_copy(3).start()

    def mixer_relay():
        m_copy(0).wait_recv()
        mpart[right, :, left_half] = (
            mpart[right, :, left_half].astype(jnp.float32) + m1[0].astype(jnp.float32)
        ).astype(jnp.bfloat16)
        m_copy(4).start()
        m_copy(1).wait_recv()
        mpart[left, :, right_half] = (
            mpart[left, :, right_half].astype(jnp.float32) + m1[1].astype(jnp.float32)
        ).astype(jnp.bfloat16)
        m_copy(5).start()

    def mixer_finish():
        for which in range(2, 6):
            m_copy(which).wait_recv()
        total = (
            mpart[tp].astype(jnp.float32)
            + m2[0].astype(jnp.float32)
            + m2[1].astype(jnp.float32)
        )
        squares = jnp.mean(total * total, axis=-1, keepdims=True)
        mixed_ref[...] = (total * lax.rsqrt(squares + norm_eps) * mix_gain_ref[...]).astype(
            jnp.bfloat16
        )

    low = pl.ds(0, half)
    high = pl.ds(half, half)

    def g_copy(k, which):
        if which == 0:
            src, dst, to = xbuf.at[k, 0], xbuf.at[k, 1], right
        elif which == 1:
            src, dst, to = xbuf.at[k, 0], xbuf.at[k, 2], left
        elif which == 2:
            src, dst, to = xbuf.at[k, 1, :, low], xbuf.at[k, 3, :, low], right
        else:
            src, dst, to = xbuf.at[k, 2, :, high], xbuf.at[k, 3, :, high], left
        return pltpu.make_async_remote_copy(
            src_ref=src,
            dst_ref=dst,
            send_sem=g_send.at[k, which],
            recv_sem=g_recv.at[k, which],
            device_id={"tp": to},
            device_id_type=MESH,
        )

    def q_copy(k, which):
        if which == 0:
            src, dst, to = pbuf.at[k, 3, :, low], r1.at[k, 0], right
        elif which == 1:
            src, dst, to = pbuf.at[k, 3, :, high], r1.at[k, 1], left
        elif which == 2:
            src, dst, to = pbuf.at[k, 2, :, high], r2.at[k, 0, :, high], right
        elif which == 3:
            src, dst, to = pbuf.at[k, 1, :, low], r2.at[k, 1, :, low], left
        elif which == 4:
            src, dst, to = pbuf.at[k, 2, :, low], r2.at[k, 0, :, low], right
        else:
            src, dst, to = pbuf.at[k, 1, :, high], r2.at[k, 1, :, high], left
        return pltpu.make_async_remote_copy(
            src_ref=src,
            dst_ref=dst,
            send_sem=q_send.at[k, which],
            recv_sem=q_recv.at[k, which],
            device_id={"tp": to},
            device_id_type=MESH,
        )

    def arrive(k):
        with jax.named_scope("arrive_wait"):
            bulk(recv, a_recv, k)
        rows = tiles_to_rows(recv[k].reshape(ROWS, 16, lanes), perm_ref[...], lanes)
        for g in range(GROUPS):
            for s in range(16):
                xbuf[k, 0, 16 * g : 16 * g + 16, lanes * s : lanes * s + lanes] = rows[g][s]
        g_copy(k, 0).start()
        g_copy(k, 1).start()

    def forward(k):
        with jax.named_scope("forward_wait"):
            g_copy(k, 0).wait_recv()
            g_copy(k, 2).start()
            g_copy(k, 1).wait_recv()
            g_copy(k, 3).start()

    def multiply(k, sends=True):
        if k == first_multiplied:
            pltpu.make_async_copy(wgu, wgu, w_sem.at[0]).wait()
            pltpu.make_async_copy(wdn, wdn, w_sem.at[1]).wait()

        with jax.named_scope("multiply_wait"):
            g_copy(k, 2).wait_recv()
            g_copy(k, 3).wait_recv()
        for n in range(gate_tiles):
            both = jnp.dot(
                xbuf[k].reshape(n_tp * ROWS, width), wgu[n], preferred_element_type=jnp.float32
            )
            gate, up = both[:, :128], both[:, 128:]
            hid[:, 128 * n : 128 * n + 128] = (gate / (1.0 + jnp.exp(-gate)) * up).astype(
                jnp.bfloat16
            )
        for n in range(down_tiles):
            part = jnp.dot(hid[...], wdn[n], preferred_element_type=jnp.float32)
            pbuf[k, :, :, 256 * n : 256 * n + 256] = part.astype(jnp.bfloat16).reshape(
                n_tp, ROWS, 256
            )
            if sends and n == down_tiles // 2 - 1:
                q_copy(k, 0).start()
        if sends:
            for which in range(1, 4):
                q_copy(k, which).start()

    def hand_on(k):
        for which in range(4):
            q_copy(k, which).start()

    def relay(k):
        with jax.named_scope("relay_wait"):
            q_copy(k, 0).wait_recv()
        pbuf[k, 2, :, low] = (
            pbuf[k, 2, :, low].astype(jnp.float32) + r1[k, 0].astype(jnp.float32)
        ).astype(jnp.bfloat16)
        q_copy(k, 4).start()
        q_copy(k, 1).wait_recv()
        pbuf[k, 1, :, high] = (
            pbuf[k, 1, :, high].astype(jnp.float32) + r1[k, 1].astype(jnp.float32)
        ).astype(jnp.bfloat16)
        q_copy(k, 5).start()

    def finish(k):
        with jax.named_scope("finish_wait"):
            for which in range(2, 6):
                q_copy(k, which).wait_recv()
        total = (
            pbuf[k, 0].astype(jnp.float32)
            + r2[k, 0].astype(jnp.float32)
            + r2[k, 1].astype(jnp.float32)
        ).astype(jnp.bfloat16)
        tiles = rows_to_tiles(total, perm_ref[...], width)
        flat = back.at[k].reshape(ROWS, 16, lanes)
        for g in range(GROUPS):
            flat[16 * g : 16 * g + 16] = tiles[g]
        if k == SELF_CHUNK:
            ret[k, yc] = back[k, yc]

        spread(b_copy, k)

    def combine(k):
        with jax.named_scope("combine_wait"):
            bulk(ret, b_recv, k)
        rows = tiles_to_rows(ret[k].reshape(ROWS, 16, lanes), perm_ref[...], lanes)
        block = jnp.concatenate([jnp.concatenate(r, axis=1) for r in rows], axis=0)
        dims = (((0,), (0,)), ((), ()))
        part = lax.dot_general(
            mix[k, 0], block, dims, preferred_element_type=jnp.float32
        ) + lax.dot_general(mix[k, 1], block, dims, preferred_element_type=jnp.float32)
        if k == last_combined:
            out_ref[...] = (acc[...] + part).astype(jnp.bfloat16)
        elif k == first_combined:
            acc[...] = part
        else:
            acc[...] += part

    stages = dict(
        D=dispatch,
        B=begin,
        S=send,
        O=mixer_own,
        H=mixer_halo,
        P=mixer_transit,
        Q=mixer_direct,
        R=mixer_relay,
        X=mixer_finish,
        A=arrive,
        F=forward,
        W=multiply,
        M=functools.partial(multiply, sends=False),
        T=hand_on,
        L=relay,
        E=finish,
        C=combine,
    )
    order = ORDER
    first_multiplied = [int(o[1]) for o in order if o[0] in "MW"][0]
    combined = [int(o[1]) for o in order if o[0] == "C"]
    first_combined, last_combined = combined[0], combined[-1]
    for op in order:
        with jax.named_scope(op):
            stages[op[0]](*(int(k) for k in op[1:]))

    def drain(k):
        bulk(outb, a_send, k)
        bulk(back, b_send, k)
        for which in range(4):
            g_copy(k, which).wait_send()
        for which in range(6):
            q_copy(k, which).wait_send()

    with jax.named_scope("drain"):
        for which in range(2):
            h_copy(which).wait_send()
        for which in range(6):
            m_copy(which).wait_send()
        for k in range(CHUNKS):
            drain(k)


def settle_kernel(mixed_ref, moe_ref, mixed_out, moe_out, sem):
    copies = [
        pltpu.make_async_copy(mixed_ref, mixed_out, sem.at[0]),
        pltpu.make_async_copy(moe_ref, moe_out, sem.at[1]),
    ]
    for copy in copies:
        copy.start()
    for copy in copies:
        copy.wait()


def settle(mixed, moe):
    hbm = pl.BlockSpec(memory_space=pl.ANY)
    vmem = pl.BlockSpec(memory_space=pltpu.VMEM)
    return pl.pallas_call(
        settle_kernel,
        out_shape=tuple(jax.ShapeDtypeStruct(a.shape, a.dtype) for a in (mixed, moe)),
        in_specs=[vmem, vmem],
        out_specs=(hbm, hbm),
        scratch_shapes=[pltpu.SemaphoreType.DMA((2,))],
        compiler_params=pltpu.CompilerParams(vmem_limit_bytes=58 * 1024 * 1024),
    )(*(pltpu.with_memory_space_constraint(a, pltpu.VMEM) for a in (mixed, moe)))


def shards(
    queries,
    key_rows,
    value_rows,
    sink_logits,
    out_weight,
    mix_gain,
    moe_tokens,
    moe_gain,
    routes,
    route_weights,
    expert_gate,
    expert_up,
    expert_down,
):
    tok, width = moe_tokens.shape
    n_tp = lax.axis_size("tp")
    hidden = expert_gate.shape[2]
    lanes = width // 16
    own_rows = queries.shape[0] // n_tp
    bf16 = jnp.bfloat16
    hbm = pl.BlockSpec(memory_space=pl.ANY)
    vmem = pl.BlockSpec(memory_space=pltpu.VMEM)
    dma = pltpu.SemaphoreType.DMA
    tiles = (CHUNKS, HALVES * N_YC, CAP, 16, lanes)
    small = (
        moe_tokens,
        moe_gain[None, :],
        routes.T,
        route_weights.T,
        queries.T,
        key_rows.T,
        value_rows.T,
        sink_logits[None, :],
        mix_gain[None, :],
    )
    mixed, moe = pl.pallas_call(
        functools.partial(layer_kernel, n_tp),
        out_shape=(pltpu.VMEM((own_rows, width), bf16), pltpu.VMEM((tok, width), bf16)),
        in_specs=[hbm] * 13,
        out_specs=(vmem, vmem),
        scratch_shapes=[
            *[pltpu.VMEM(a.shape, a.dtype) for a in small],
            pltpu.VMEM(tiles, bf16),
            pltpu.VMEM(tiles, bf16),
            pltpu.VMEM((CHUNKS, n_tp, ROWS, width), bf16),
            pltpu.VMEM((CHUNKS, n_tp, ROWS, width), bf16),
            pltpu.VMEM((CHUNKS, 2, ROWS, width // 2), bf16),
            pltpu.VMEM((CHUNKS, 2, ROWS, width), bf16),
            pltpu.VMEM(tiles, bf16),
            pltpu.VMEM(tiles, bf16),
            pltpu.VMEM((hidden // 128, width, 256), bf16),
            pltpu.VMEM((width // 256, hidden, 256), bf16),
            pltpu.VMEM((n_tp * ROWS, hidden), bf16),
            pltpu.VMEM((tok, width), jnp.float32),
            pltpu.VMEM((CHUNKS, 2, ROWS, tok), bf16),
            pltpu.VMEM((256, 256), bf16),
            pltpu.VMEM((tok, width), bf16),
            pltpu.VMEM((2, HDIM, WINDOW), bf16),
            pltpu.VMEM((queries.shape[1], queries.shape[0]), bf16),
            pltpu.VMEM(out_weight.shape, bf16),
            pltpu.VMEM((n_tp, own_rows, width), bf16),
            pltpu.VMEM((2, own_rows, width // 2), bf16),
            pltpu.VMEM((2, own_rows, width), bf16),
            dma((len(small),)),
            dma((2,)),
            dma((2,)),
            dma((6,)),
            dma((6,)),
            dma((3,)),
            dma((CHUNKS,)),
            dma((CHUNKS,)),
            dma((CHUNKS, 4)),
            dma((CHUNKS, 4)),
            dma((CHUNKS, 6)),
            dma((CHUNKS, 6)),
            dma((CHUNKS,)),
            dma((CHUNKS,)),
        ],
        compiler_params=pltpu.CompilerParams(
            collective_id=0, has_side_effects=True, vmem_limit_bytes=58 * 1024 * 1024
        ),
    )(*small, expert_gate, expert_up, expert_down, out_weight)
    return settle(mixed, moe)


def solution(mesh):
    return jax.shard_map(
        shards,
        mesh=mesh,
        in_specs=(
            P("ep", "tp"),
            P("ep", "tp"),
            P("ep", "tp"),
            P("tp"),
            P("tp", None),
            P(),
            P(("ep", "tp"), None),
            P(),
            P(("ep", "tp"), None),
            P(("ep", "tp"), None),
            P("ep", None, "tp"),
            P("ep", None, "tp"),
            P("ep", "tp", None),
        ),
        out_specs=(P(("ep", "tp"), None), P(("ep", "tp"), None)),
        check_vma=False,
    )
```

```python
import functools

import jax
import jax.numpy as jnp
from jax import lax
from jax.experimental import pallas as pl
from jax.experimental.pallas import tpu as pltpu
from jax.sharding import PartitionSpec as P

HDIM = 64
WINDOW = 128
MESH = pl.DeviceIdType.MESH

norm_eps = 1e-06
masked_value = -1e30

N_Z = 8
N_YC = 8
CAP = 5
CHUNKS = 4
HALVES = 2
OFFSETS = ((2, 6), (3, 5), (4, 7), (0, 1))
SELF_CHUNK = 3
ORDER = (
    "D3", "B", "S3", "D0", "S0", "O", "H", "P", "D1", "D2", "A3", "S1", "A0", "F3", "S2", "A1",
    "F0", "M3", "F1", "A2", "W1", "M0", "F2", "L1", "T0", "M2", "E1", "L0", "T2", "E0", "L2", "T3",
    "C1", "E2", "L3", "R", "Q", "C0", "E3", "C2", "X", "C3",
)
ROWS = HALVES * N_YC * CAP
GROUPS = ROWS // 16


def rows_to_tiles(block, perm, width):
    lanes = width // 16
    stacked = jnp.concatenate(
        [
            jnp.concatenate(
                [block[16 * g : 16 * g + 16, lanes * s : lanes * s + lanes] for s in range(16)],
                axis=0,
            )
            for g in range(GROUPS)
        ],
        axis=1,
    )
    turned = jnp.dot(perm, stacked, preferred_element_type=jnp.float32).astype(jnp.bfloat16)
    return [turned[:, lanes * g : lanes * g + lanes].reshape(16, 16, lanes) for g in range(GROUPS)]


def tiles_to_rows(tiles, perm, lanes):
    stacked = jnp.concatenate(
        [tiles[16 * g : 16 * g + 16].reshape(256, lanes) for g in range(GROUPS)], axis=1
    )
    turned = jnp.dot(perm, stacked, preferred_element_type=jnp.float32).astype(jnp.bfloat16)
    return [
        [turned[16 * s : 16 * s + 16, lanes * g : lanes * g + lanes] for s in range(16)]
        for g in range(GROUPS)
    ]


def layer_kernel(
    n_tp,
    tokens_in,
    gain_in,
    routes_in,
    weights_in,
    queries_in,
    keys_in,
    values_in,
    sink_in,
    mix_gain_in,
    gate_ref,
    up_ref,
    down_ref,
    project_ref,
    mixed_ref,
    out_ref,
    tokens_ref,
    gain_ref,
    routes_ref,
    weights_ref,
    queries_ref,
    keys_ref,
    values_ref,
    sink_ref,
    mix_gain_ref,
    outb,
    recv,
    xbuf,
    pbuf,
    r1,
    r2,
    back,
    ret,
    wgu,
    wdn,
    hid,
    acc,
    mix,
    perm_ref,
    row_ref,
    halo,
    attended,
    wproj,
    mpart,
    m1,
    m2,
    i_sem,
    h_send,
    h_recv,
    m_send,
    m_recv,
    w_sem,
    a_send,
    a_recv,
    g_send,
    g_recv,
    q_send,
    q_recv,
    b_send,
    b_recv,
):
    width = tokens_ref.shape[1]
    half = width // 2
    lanes = width // 16
    gate_tiles = wgu.shape[0]
    down_tiles = wdn.shape[0]
    me = lax.axis_index("ep")
    tp = lax.axis_index("tp")
    z = lax.div(me, jnp.int32(N_YC))
    yc = lax.rem(me, jnp.int32(N_YC))
    right = lax.rem(tp + 1, jnp.int32(n_tp))
    left = lax.rem(tp + n_tp - 1, jnp.int32(n_tp))

    inputs = (
        (routes_in, routes_ref),
        (tokens_in, tokens_ref),
        (gain_in, gain_ref),
        (weights_in, weights_ref),
        (keys_in, keys_ref),
        (values_in, values_ref),
        (queries_in, queries_ref),
        (sink_in, sink_ref),
        (mix_gain_in, mix_gain_ref),
    )
    for n, (src, dst) in enumerate(inputs):
        pltpu.make_async_copy(src, dst, i_sem.at[n]).start()

    barrier = pltpu.get_barrier_semaphore()

    n_ep = N_Z * N_YC

    def greet(i, carry):
        ahead = lax.rem(me + n_ep // 2 + i, jnp.int32(n_ep))
        behind = lax.rem(me + n_ep // 2 - 1 - i + n_ep, jnp.int32(n_ep))
        pl.semaphore_signal(barrier, inc=1, device_id={"ep": ahead}, device_id_type=MESH)

        @pl.when(behind != me)
        def _():
            pl.semaphore_signal(barrier, inc=1, device_id={"ep": behind}, device_id_type=MESH)

        return carry

    lax.fori_loop(0, n_ep // 2, greet, 0)
    pl.semaphore_signal(barrier, inc=1, device_id={"tp": right}, device_id_type=MESH)
    pl.semaphore_signal(barrier, inc=1, device_id={"tp": left}, device_id_type=MESH)

    for n in range(gate_tiles):
        for part, ref in enumerate((gate_ref, up_ref)):
            pltpu.make_async_copy(
                ref.at[0, :, pl.ds(128 * n, 128)], wgu.at[n, :, pl.ds(128 * part, 128)], w_sem.at[0]
            ).start()
    for n in range(down_tiles):
        pltpu.make_async_copy(
            down_ref.at[0, :, pl.ds(256 * n, 256)], wdn.at[n], w_sem.at[1]
        ).start()

    pltpu.make_async_copy(project_ref, wproj, w_sem.at[2]).start()

    for n, (src, dst) in enumerate(inputs):
        pltpu.make_async_copy(src, dst, i_sem.at[n]).wait()

    tok = tokens_ref.shape[0]
    e_rows = [routes_ref[0:1, :], routes_ref[1:2, :]]
    expert_id = lax.broadcasted_iota(jnp.int32, (N_Z * N_YC, tok), 0)
    named = [jnp.where(expert_id == e, 1.0, 0.0) for e in e_rows]
    before = jnp.where(
        lax.broadcasted_iota(jnp.int32, (tok, tok), 0)
        < lax.broadcasted_iota(jnp.int32, (tok, tok), 1),
        1.0,
        0.0,
    ).astype(jnp.bfloat16)
    ranks = [
        jnp.dot(n.astype(jnp.bfloat16), before, preferred_element_type=jnp.float32) for n in named
    ]
    ranks[1] = ranks[1] + jnp.sum(named[0], axis=1, keepdims=True)
    slots = []
    flat_offsets = [o for pair in OFFSETS for o in pair]
    for e, n, r in zip(e_rows, named, ranks):
        rank = jnp.sum(n * r, axis=0, keepdims=True).astype(jnp.int32)
        offset = (lax.shift_right_logical(e, 3) - z) & (N_Z - 1)
        place = jnp.zeros_like(offset)
        for p, o in enumerate(flat_offsets):
            place = jnp.where(offset == o, p, place)
        slots.append((place * N_YC + (e & (N_YC - 1))) * CAP + rank)

    i256 = lax.broadcasted_iota(jnp.int32, (256, 256), 0)
    j256 = lax.broadcasted_iota(jnp.int32, (256, 256), 1)
    perm_ref[...] = jnp.where(
        j256 == (i256 & 15) * 16 + lax.shift_right_logical(i256, 4), 1.0, 0.0
    ).astype(jnp.bfloat16)

    x = tokens_ref[...].astype(jnp.float32)
    squares = jnp.mean(x * x, axis=-1, keepdims=True)
    row_ref[...] = (x * lax.rsqrt(squares + norm_eps) * gain_ref[...]).astype(jnp.bfloat16)

    def peer(i, y, sign, k):
        return lax.rem(z + (sign * OFFSETS[k][i]) % N_Z, jnp.int32(N_Z)) * N_YC + y

    def a_copy(k, i, y):
        return pltpu.make_async_remote_copy(
            src_ref=outb.at[k, i * N_YC + y],
            dst_ref=recv.at[k, i * N_YC + yc],
            send_sem=a_send.at[k],
            recv_sem=a_recv.at[k],
            device_id={"ep": peer(i, y, 1, k)},
            device_id_type=MESH,
        )

    def b_copy(k, i, y):
        return pltpu.make_async_remote_copy(
            src_ref=back.at[k, i * N_YC + y],
            dst_ref=ret.at[k, i * N_YC + yc],
            send_sem=b_send.at[k],
            recv_sem=b_recv.at[k],
            device_id={"ep": peer(i, y, -1, k)},
            device_id_type=MESH,
        )

    def spread(copy_of, k):
        def one(j, carry, halves):
            y = (yc + N_YC // 2 + j) & (N_YC - 1)
            for i in halves:
                if OFFSETS[k][i] == 0:

                    @pl.when(y != yc)
                    def _():
                        copy_of(k, i, y).start()
                else:
                    copy_of(k, i, y).start()
            return carry

        for halves in ((1,), (0,)) if k == SELF_CHUNK else ((0, 1),):
            lax.fori_loop(0, N_YC, functools.partial(one, halves=halves), 0)

    def bulk(buffer, sem, k):
        count = HALVES * N_YC - (k == SELF_CHUNK)
        view = buffer.at[k, pl.ds(0, count)]
        pltpu.make_async_copy(view, view, sem.at[k]).wait()

    def dispatch(k):
        row_id = lax.broadcasted_iota(jnp.int32, (ROWS, tok), 0) + k * ROWS
        hits = [row_id == s for s in slots]
        select = jnp.where(jnp.logical_or(hits[0], hits[1]), 1.0, 0.0).astype(jnp.bfloat16)
        shares = jnp.where(hits[0], weights_ref[0:1, :], 0.0) + jnp.where(
            hits[1], weights_ref[1:2, :], 0.0
        )
        coarse = shares.astype(jnp.bfloat16)
        mix[k, 0] = coarse
        mix[k, 1] = (shares - coarse.astype(jnp.float32)).astype(jnp.bfloat16)
        block = jnp.dot(select, row_ref[...], preferred_element_type=jnp.float32)
        tiles = rows_to_tiles(block.astype(jnp.bfloat16), perm_ref[...], width)
        flat = outb.at[k].reshape(ROWS, 16, lanes)
        for g in range(GROUPS):
            flat[16 * g : 16 * g + 16] = tiles[g]
        if k == SELF_CHUNK:
            recv[k, yc] = outb[k, yc]

    follower = lax.rem(me + 1, jnp.int32(N_Z * N_YC))

    def h_copy(which):
        ref = (keys_ref, values_ref)[which]
        return pltpu.make_async_remote_copy(
            src_ref=ref.at[:, pl.ds(ref.shape[1] - WINDOW, WINDOW)],
            dst_ref=halo.at[which],
            send_sem=h_send.at[which],
            recv_sem=h_recv.at[which],
            device_id={"ep": follower},
            device_id_type=MESH,
        )

    def begin():
        pl.semaphore_wait(barrier, n_ep - 1 + 2)
        h_copy(0).start()
        h_copy(1).start()

    def send(k):
        spread(a_copy, k)

    heads = queries_ref.shape[0] // HDIM
    sinks = jnp.concatenate(
        [jnp.broadcast_to(sink_ref[0:1, h : h + 1], (1, WINDOW)) for h in range(heads)], axis=1
    )
    key_i = lax.broadcasted_iota(jnp.int32, (2 * WINDOW, heads * WINDOW), 0)
    query_i = lax.broadcasted_iota(jnp.int32, (2 * WINDOW, heads * WINDOW), 1) & (WINDOW - 1)
    in_window = jnp.logical_and(key_i > query_i, key_i <= query_i + WINDOW)

    def attend(b, keys, values, allowed):
        at = slice(WINDOW * b, WINDOW * b + WINDOW)
        block = jnp.concatenate(
            [queries_ref[HDIM * h : HDIM * h + HDIM, at] for h in range(heads)], axis=1
        )
        scores = lax.dot_general(
            keys, block, (((0,), (0,)), ((), ())), preferred_element_type=jnp.float32
        ) * HDIM ** (-0.5)
        logits = jnp.where(allowed, scores, masked_value)
        top = jnp.maximum(jnp.max(logits, axis=0, keepdims=True), sinks)
        exponent = jnp.exp(logits - top)
        denominator = jnp.sum(exponent, axis=0, keepdims=True) + jnp.exp(sinks - top)
        probs = (exponent / denominator).astype(jnp.bfloat16)
        result = jnp.dot(values, probs, preferred_element_type=jnp.float32).astype(jnp.bfloat16)
        for h in range(heads):
            attended[HDIM * h : HDIM * h + HDIM, at] = result[:, WINDOW * h : WINDOW * h + WINDOW]

    blocks = queries_ref.shape[1] // WINDOW
    own_rows = mpart.shape[1]
    block_parts = WINDOW // own_rows

    def project(b):
        at_rows = slice(WINDOW * b, WINDOW * b + WINDOW)
        for n in range(width // 512):
            at = slice(512 * n, 512 * n + 512)
            part = lax.dot_general(
                attended[:, at_rows],
                wproj[:, at],
                (((0,), (0,)), ((), ())),
                preferred_element_type=jnp.float32,
            ).astype(jnp.bfloat16)
            mpart[block_parts * b : block_parts * b + block_parts, :, at] = part.reshape(
                block_parts, own_rows, 512
            )

    def mixer_own():
        for b in range(1, blocks):
            at = slice(WINDOW * (b - 1), WINDOW * (b + 1))
            attend(b, keys_ref[:, at], values_ref[:, at], in_window)
        pltpu.make_async_copy(wproj, wproj, w_sem.at[2]).wait()
        for b in range(1, blocks):
            project(b)

    def mixer_halo():
        with jax.named_scope("halo_wait"):
            h_copy(0).wait_recv()
            h_copy(1).wait_recv()
        first = slice(0, WINDOW)
        attend(
            0,
            jnp.concatenate([halo[0], keys_ref[:, first]], axis=1),
            jnp.concatenate([halo[1], values_ref[:, first]], axis=1),
            jnp.logical_and(in_window, jnp.logical_or(key_i >= WINDOW, me > 0)),
        )
        project(0)

    across = lax.rem(tp + 2, jnp.int32(n_tp))
    left_half = pl.ds(0, half)
    right_half = pl.ds(half, half)

    def m_copy(which):
        if which == 0:
            src, dst, to = mpart.at[across, :, left_half], m1.at[0], right
        elif which == 1:
            src, dst, to = mpart.at[across, :, right_half], m1.at[1], left
        elif which == 2:
            src, dst, to = mpart.at[right, :, right_half], m2.at[0, :, right_half], right
        elif which == 3:
            src, dst, to = mpart.at[left, :, left_half], m2.at[1, :, left_half], left
        elif which == 4:
            src, dst, to = mpart.at[right, :, left_half], m2.at[0, :, left_half], right
        else:
            src, dst, to = mpart.at[left, :, right_half], m2.at[1, :, right_half], left
        return pltpu.make_async_remote_copy(
            src_ref=src,
            dst_ref=dst,
            send_sem=m_send.at[which],
            recv_sem=m_recv.at[which],
            device_id={"tp": to},
            device_id_type=MESH,
        )

    def mixer_transit():
        m_copy(0).start()
        m_copy(1).start()

    def mixer_direct():
        m_copy(2).start()
        m_copy(3).start()

    def mixer_relay():
        m_copy(0).wait_recv()
        mpart[right, :, left_half] = (
            mpart[right, :, left_half].astype(jnp.float32) + m1[0].astype(jnp.float32)
        ).astype(jnp.bfloat16)
        m_copy(4).start()
        m_copy(1).wait_recv()
        mpart[left, :, right_half] = (
            mpart[left, :, right_half].astype(jnp.float32) + m1[1].astype(jnp.float32)
        ).astype(jnp.bfloat16)
        m_copy(5).start()

    def mixer_finish():
        for which in range(2, 6):
            m_copy(which).wait_recv()
        total = (
            mpart[tp].astype(jnp.float32)
            + m2[0].astype(jnp.float32)
            + m2[1].astype(jnp.float32)
        )
        squares = jnp.mean(total * total, axis=-1, keepdims=True)
        mixed_ref[...] = (total * lax.rsqrt(squares + norm_eps) * mix_gain_ref[...]).astype(
            jnp.bfloat16
        )

    low = pl.ds(0, half)
    high = pl.ds(half, half)

    def g_copy(k, which):
        if which == 0:
            src, dst, to = xbuf.at[k, 0], xbuf.at[k, 1], right
        elif which == 1:
            src, dst, to = xbuf.at[k, 0], xbuf.at[k, 2], left
        elif which == 2:
            src, dst, to = xbuf.at[k, 1, :, low], xbuf.at[k, 3, :, low], right
        else:
            src, dst, to = xbuf.at[k, 2, :, high], xbuf.at[k, 3, :, high], left
        return pltpu.make_async_remote_copy(
            src_ref=src,
            dst_ref=dst,
            send_sem=g_send.at[k, which],
            recv_sem=g_recv.at[k, which],
            device_id={"tp": to},
            device_id_type=MESH,
        )

    def q_copy(k, which):
        if which == 0:
            src, dst, to = pbuf.at[k, 3, :, low], r1.at[k, 0], right
        elif which == 1:
            src, dst, to = pbuf.at[k, 3, :, high], r1.at[k, 1], left
        elif which == 2:
            src, dst, to = pbuf.at[k, 2, :, high], r2.at[k, 0, :, high], right
        elif which == 3:
            src, dst, to = pbuf.at[k, 1, :, low], r2.at[k, 1, :, low], left
        elif which == 4:
            src, dst, to = pbuf.at[k, 2, :, low], r2.at[k, 0, :, low], right
        else:
            src, dst, to = pbuf.at[k, 1, :, high], r2.at[k, 1, :, high], left
        return pltpu.make_async_remote_copy(
            src_ref=src,
            dst_ref=dst,
            send_sem=q_send.at[k, which],
            recv_sem=q_recv.at[k, which],
            device_id={"tp": to},
            device_id_type=MESH,
        )

    def arrive(k):
        with jax.named_scope("arrive_wait"):
            bulk(recv, a_recv, k)
        rows = tiles_to_rows(recv[k].reshape(ROWS, 16, lanes), perm_ref[...], lanes)
        for g in range(GROUPS):
            for s in range(16):
                xbuf[k, 0, 16 * g : 16 * g + 16, lanes * s : lanes * s + lanes] = rows[g][s]
        g_copy(k, 0).start()
        g_copy(k, 1).start()

    def forward(k):
        with jax.named_scope("forward_wait"):
            g_copy(k, 0).wait_recv()
            g_copy(k, 2).start()
            g_copy(k, 1).wait_recv()
            g_copy(k, 3).start()

    def multiply(k, sends=True):
        if k == first_multiplied:
            pltpu.make_async_copy(wgu, wgu, w_sem.at[0]).wait()
            pltpu.make_async_copy(wdn, wdn, w_sem.at[1]).wait()

        with jax.named_scope("multiply_wait"):
            g_copy(k, 2).wait_recv()
            g_copy(k, 3).wait_recv()
        for n in range(gate_tiles):
            both = jnp.dot(
                xbuf[k].reshape(n_tp * ROWS, width), wgu[n], preferred_element_type=jnp.float32
            )
            gate, up = both[:, :128], both[:, 128:]
            hid[:, 128 * n : 128 * n + 128] = (gate / (1.0 + jnp.exp(-gate)) * up).astype(
                jnp.bfloat16
            )
        for n in range(down_tiles):
            part = jnp.dot(hid[...], wdn[n], preferred_element_type=jnp.float32)
            pbuf[k, :, :, 256 * n : 256 * n + 256] = part.astype(jnp.bfloat16).reshape(
                n_tp, ROWS, 256
            )
            if sends and n == down_tiles // 2 - 1:
                q_copy(k, 0).start()
        if sends:
            for which in range(1, 4):
                q_copy(k, which).start()

    def hand_on(k):
        for which in range(4):
            q_copy(k, which).start()

    def relay(k):
        with jax.named_scope("relay_wait"):
            q_copy(k, 0).wait_recv()
        pbuf[k, 2, :, low] = (
            pbuf[k, 2, :, low].astype(jnp.float32) + r1[k, 0].astype(jnp.float32)
        ).astype(jnp.bfloat16)
        q_copy(k, 4).start()
        q_copy(k, 1).wait_recv()
        pbuf[k, 1, :, high] = (
            pbuf[k, 1, :, high].astype(jnp.float32) + r1[k, 1].astype(jnp.float32)
        ).astype(jnp.bfloat16)
        q_copy(k, 5).start()

    def finish(k):
        with jax.named_scope("finish_wait"):
            for which in range(2, 6):
                q_copy(k, which).wait_recv()
        total = (
            pbuf[k, 0].astype(jnp.float32)
            + r2[k, 0].astype(jnp.float32)
            + r2[k, 1].astype(jnp.float32)
        ).astype(jnp.bfloat16)
        tiles = rows_to_tiles(total, perm_ref[...], width)
        flat = back.at[k].reshape(ROWS, 16, lanes)
        for g in range(GROUPS):
            flat[16 * g : 16 * g + 16] = tiles[g]
        if k == SELF_CHUNK:
            ret[k, yc] = back[k, yc]

        spread(b_copy, k)

    def combine(k):
        with jax.named_scope("combine_wait"):
            bulk(ret, b_recv, k)
        rows = tiles_to_rows(ret[k].reshape(ROWS, 16, lanes), perm_ref[...], lanes)
        block = jnp.concatenate([jnp.concatenate(r, axis=1) for r in rows], axis=0)
        dims = (((0,), (0,)), ((), ()))
        part = lax.dot_general(
            mix[k, 0], block, dims, preferred_element_type=jnp.float32
        ) + lax.dot_general(mix[k, 1], block, dims, preferred_element_type=jnp.float32)
        if k == last_combined:
            out_ref[...] = (acc[...] + part).astype(jnp.bfloat16)
        elif k == first_combined:
            acc[...] = part
        else:
            acc[...] += part

    stages = dict(
        D=dispatch,
        B=begin,
        S=send,
        O=mixer_own,
        H=mixer_halo,
        P=mixer_transit,
        Q=mixer_direct,
        R=mixer_relay,
        X=mixer_finish,
        A=arrive,
        F=forward,
        W=multiply,
        M=functools.partial(multiply, sends=False),
        T=hand_on,
        L=relay,
        E=finish,
        C=combine,
    )
    order = ORDER
    first_multiplied = [int(o[1]) for o in order if o[0] in "MW"][0]
    combined = [int(o[1]) for o in order if o[0] == "C"]
    first_combined, last_combined = combined[0], combined[-1]
    for op in order:
        with jax.named_scope(op):
            stages[op[0]](*(int(k) for k in op[1:]))

    def drain(k):
        bulk(outb, a_send, k)
        bulk(back, b_send, k)
        for which in range(4):
            g_copy(k, which).wait_send()
        for which in range(6):
            q_copy(k, which).wait_send()

    with jax.named_scope("drain"):
        for which in range(2):
            h_copy(which).wait_send()
        for which in range(6):
            m_copy(which).wait_send()
        for k in range(CHUNKS):
            drain(k)


def settle_kernel(mixed_ref, moe_ref, mixed_out, moe_out, sem):
    copies = [
        pltpu.make_async_copy(mixed_ref, mixed_out, sem.at[0]),
        pltpu.make_async_copy(moe_ref, moe_out, sem.at[1]),
    ]
    for copy in copies:
        copy.start()
    for copy in copies:
        copy.wait()


def settle(mixed, moe):
    hbm = pl.BlockSpec(memory_space=pl.ANY)
    vmem = pl.BlockSpec(memory_space=pltpu.VMEM)
    return pl.pallas_call(
        settle_kernel,
        out_shape=tuple(jax.ShapeDtypeStruct(a.shape, a.dtype) for a in (mixed, moe)),
        in_specs=[vmem, vmem],
        out_specs=(hbm, hbm),
        scratch_shapes=[pltpu.SemaphoreType.DMA((2,))],
        compiler_params=pltpu.CompilerParams(vmem_limit_bytes=58 * 1024 * 1024),
    )(*(pltpu.with_memory_space_constraint(a, pltpu.VMEM) for a in (mixed, moe)))


def shards(
    queries,
    key_rows,
    value_rows,
    sink_logits,
    out_weight,
    mix_gain,
    moe_tokens,
    moe_gain,
    routes,
    route_weights,
    expert_gate,
    expert_up,
    expert_down,
):
    tok, width = moe_tokens.shape
    n_tp = lax.axis_size("tp")
    hidden = expert_gate.shape[2]
    lanes = width // 16
    own_rows = queries.shape[0] // n_tp
    bf16 = jnp.bfloat16
    hbm = pl.BlockSpec(memory_space=pl.ANY)
    vmem = pl.BlockSpec(memory_space=pltpu.VMEM)
    dma = pltpu.SemaphoreType.DMA
    tiles = (CHUNKS, HALVES * N_YC, CAP, 16, lanes)
    small = (
        moe_tokens,
        moe_gain[None, :],
        routes.T,
        route_weights.T,
        queries.T,
        key_rows.T,
        value_rows.T,
        sink_logits[None, :],
        mix_gain[None, :],
    )
    mixed, moe = pl.pallas_call(
        functools.partial(layer_kernel, n_tp),
        out_shape=(pltpu.VMEM((own_rows, width), bf16), pltpu.VMEM((tok, width), bf16)),
        in_specs=[hbm] * 13,
        out_specs=(vmem, vmem),
        scratch_shapes=[
            *[pltpu.VMEM(a.shape, a.dtype) for a in small],
            pltpu.VMEM(tiles, bf16),
            pltpu.VMEM(tiles, bf16),
            pltpu.VMEM((CHUNKS, n_tp, ROWS, width), bf16),
            pltpu.VMEM((CHUNKS, n_tp, ROWS, width), bf16),
            pltpu.VMEM((CHUNKS, 2, ROWS, width // 2), bf16),
            pltpu.VMEM((CHUNKS, 2, ROWS, width), bf16),
            pltpu.VMEM(tiles, bf16),
            pltpu.VMEM(tiles, bf16),
            pltpu.VMEM((hidden // 128, width, 256), bf16),
            pltpu.VMEM((width // 256, hidden, 256), bf16),
            pltpu.VMEM((n_tp * ROWS, hidden), bf16),
            pltpu.VMEM((tok, width), jnp.float32),
            pltpu.VMEM((CHUNKS, 2, ROWS, tok), bf16),
            pltpu.VMEM((256, 256), bf16),
            pltpu.VMEM((tok, width), bf16),
            pltpu.VMEM((2, HDIM, WINDOW), bf16),
            pltpu.VMEM((queries.shape[1], queries.shape[0]), bf16),
            pltpu.VMEM(out_weight.shape, bf16),
            pltpu.VMEM((n_tp, own_rows, width), bf16),
            pltpu.VMEM((2, own_rows, width // 2), bf16),
            pltpu.VMEM((2, own_rows, width), bf16),
            dma((len(small),)),
            dma((2,)),
            dma((2,)),
            dma((6,)),
            dma((6,)),
            dma((3,)),
            dma((CHUNKS,)),
            dma((CHUNKS,)),
            dma((CHUNKS, 4)),
            dma((CHUNKS, 4)),
            dma((CHUNKS, 6)),
            dma((CHUNKS, 6)),
            dma((CHUNKS,)),
            dma((CHUNKS,)),
        ],
        compiler_params=pltpu.CompilerParams(
            collective_id=0, has_side_effects=True, vmem_limit_bytes=58 * 1024 * 1024
        ),
    )(*small, expert_gate, expert_up, expert_down, out_weight)
    return settle(mixed, moe)


def solution(mesh):
    return jax.shard_map(
        shards,
        mesh=mesh,
        in_specs=(
            P("ep", "tp"),
            P("ep", "tp"),
            P("ep", "tp"),
            P("tp"),
            P("tp", None),
            P(),
            P(("ep", "tp"), None),
            P(),
            P(("ep", "tp"), None),
            P(("ep", "tp"), None),
            P("ep", None, "tp"),
            P("ep", None, "tp"),
            P("ep", "tp", None),
        ),
        out_specs=(P(("ep", "tp"), None), P(("ep", "tp"), None)),
        check_vma=False,
    )
```

```python
import functools

import jax
import jax.numpy as jnp
from jax import lax
from jax.experimental import pallas as pl
from jax.experimental.pallas import tpu as pltpu
from jax.sharding import PartitionSpec as P

HDIM = 64
WINDOW = 128
MESH = pl.DeviceIdType.MESH

norm_eps = 1e-06
masked_value = -1e30

N_Z = 8
N_YC = 8
CAP = 5
CHUNKS = 4
HALVES = 2
OFFSETS = ((2, 6), (3, 5), (4, 7), (0, 1))
SELF_CHUNK = 3
ORDER = (
    "D3", "D0", "B", "S3", "S0", "O", "H", "P", "D1", "D2", "A3", "S1", "A0", "F3", "S2", "A1",
    "F0", "M3", "F1", "A2", "W1", "M0", "F2", "L1", "T0", "M2", "E1", "L0", "T2", "E0", "L2", "T3",
    "C1", "E2", "L3", "R", "Q", "C0", "E3", "C2", "X", "C3",
)
ROWS = HALVES * N_YC * CAP
GROUPS = ROWS // 16


def rows_to_tiles(block, perm, width):
    lanes = width // 16
    stacked = jnp.concatenate(
        [
            jnp.concatenate(
                [block[16 * g : 16 * g + 16, lanes * s : lanes * s + lanes] for s in range(16)],
                axis=0,
            )
            for g in range(GROUPS)
        ],
        axis=1,
    )
    turned = jnp.dot(perm, stacked, preferred_element_type=jnp.float32).astype(jnp.bfloat16)
    return [turned[:, lanes * g : lanes * g + lanes].reshape(16, 16, lanes) for g in range(GROUPS)]


def tiles_to_rows(tiles, perm, lanes):
    stacked = jnp.concatenate(
        [tiles[16 * g : 16 * g + 16].reshape(256, lanes) for g in range(GROUPS)], axis=1
    )
    turned = jnp.dot(perm, stacked, preferred_element_type=jnp.float32).astype(jnp.bfloat16)
    return [
        [turned[16 * s : 16 * s + 16, lanes * g : lanes * g + lanes] for s in range(16)]
        for g in range(GROUPS)
    ]


def layer_kernel(
    n_tp,
    tokens_in,
    gain_in,
    routes_in,
    weights_in,
    queries_in,
    keys_in,
    values_in,
    sink_in,
    mix_gain_in,
    gate_ref,
    up_ref,
    down_ref,
    project_ref,
    mixed_ref,
    out_ref,
    tokens_ref,
    gain_ref,
    routes_ref,
    weights_ref,
    queries_ref,
    keys_ref,
    values_ref,
    sink_ref,
    mix_gain_ref,
    outb,
    recv,
    xbuf,
    pbuf,
    r1,
    r2,
    back,
    ret,
    wgu,
    wdn,
    hid,
    acc,
    mix,
    perm_ref,
    row_ref,
    halo,
    attended,
    wproj,
    mpart,
    m1,
    m2,
    i_sem,
    h_send,
    h_recv,
    m_send,
    m_recv,
    w_sem,
    a_send,
    a_recv,
    g_send,
    g_recv,
    q_send,
    q_recv,
    b_send,
    b_recv,
):
    width = tokens_ref.shape[1]
    half = width // 2
    lanes = width // 16
    gate_tiles = wgu.shape[0]
    down_tiles = wdn.shape[0]
    me = lax.axis_index("ep")
    tp = lax.axis_index("tp")
    z = lax.div(me, jnp.int32(N_YC))
    yc = lax.rem(me, jnp.int32(N_YC))
    right = lax.rem(tp + 1, jnp.int32(n_tp))
    left = lax.rem(tp + n_tp - 1, jnp.int32(n_tp))

    inputs = (
        (routes_in, routes_ref),
        (tokens_in, tokens_ref),
        (gain_in, gain_ref),
        (weights_in, weights_ref),
        (keys_in, keys_ref),
        (values_in, values_ref),
        (queries_in, queries_ref),
        (sink_in, sink_ref),
        (mix_gain_in, mix_gain_ref),
    )
    for n, (src, dst) in enumerate(inputs):
        pltpu.make_async_copy(src, dst, i_sem.at[n]).start()

    barrier = pltpu.get_barrier_semaphore()

    n_ep = N_Z * N_YC

    def greet(i, carry):
        ahead = lax.rem(me + n_ep // 2 + i, jnp.int32(n_ep))
        behind = lax.rem(me + n_ep // 2 - 1 - i + n_ep, jnp.int32(n_ep))
        pl.semaphore_signal(barrier, inc=1, device_id={"ep": ahead}, device_id_type=MESH)

        @pl.when(behind != me)
        def _():
            pl.semaphore_signal(barrier, inc=1, device_id={"ep": behind}, device_id_type=MESH)

        return carry

    lax.fori_loop(0, n_ep // 2, greet, 0)
    pl.semaphore_signal(barrier, inc=1, device_id={"tp": right}, device_id_type=MESH)
    pl.semaphore_signal(barrier, inc=1, device_id={"tp": left}, device_id_type=MESH)

    for n in range(gate_tiles):
        for part, ref in enumerate((gate_ref, up_ref)):
            pltpu.make_async_copy(
                ref.at[0, :, pl.ds(128 * n, 128)], wgu.at[n, :, pl.ds(128 * part, 128)], w_sem.at[0]
            ).start()
    for n in range(down_tiles):
        pltpu.make_async_copy(
            down_ref.at[0, :, pl.ds(256 * n, 256)], wdn.at[n], w_sem.at[1]
        ).start()

    pltpu.make_async_copy(project_ref, wproj, w_sem.at[2]).start()

    for n, (src, dst) in enumerate(inputs):
        pltpu.make_async_copy(src, dst, i_sem.at[n]).wait()

    tok = tokens_ref.shape[0]
    e_rows = [routes_ref[0:1, :], routes_ref[1:2, :]]
    expert_id = lax.broadcasted_iota(jnp.int32, (N_Z * N_YC, tok), 0)
    named = [jnp.where(expert_id == e, 1.0, 0.0) for e in e_rows]
    before = jnp.where(
        lax.broadcasted_iota(jnp.int32, (tok, tok), 0)
        < lax.broadcasted_iota(jnp.int32, (tok, tok), 1),
        1.0,
        0.0,
    ).astype(jnp.bfloat16)
    ranks = [
        jnp.dot(n.astype(jnp.bfloat16), before, preferred_element_type=jnp.float32) for n in named
    ]
    ranks[1] = ranks[1] + jnp.sum(named[0], axis=1, keepdims=True)
    slots = []
    flat_offsets = [o for pair in OFFSETS for o in pair]
    for e, n, r in zip(e_rows, named, ranks):
        rank = jnp.sum(n * r, axis=0, keepdims=True).astype(jnp.int32)
        offset = (lax.shift_right_logical(e, 3) - z) & (N_Z - 1)
        place = jnp.zeros_like(offset)
        for p, o in enumerate(flat_offsets):
            place = jnp.where(offset == o, p, place)
        slots.append((place * N_YC + (e & (N_YC - 1))) * CAP + rank)

    i256 = lax.broadcasted_iota(jnp.int32, (256, 256), 0)
    j256 = lax.broadcasted_iota(jnp.int32, (256, 256), 1)
    perm_ref[...] = jnp.where(
        j256 == (i256 & 15) * 16 + lax.shift_right_logical(i256, 4), 1.0, 0.0
    ).astype(jnp.bfloat16)

    x = tokens_ref[...].astype(jnp.float32)
    squares = jnp.mean(x * x, axis=-1, keepdims=True)
    row_ref[...] = (x * lax.rsqrt(squares + norm_eps) * gain_ref[...]).astype(jnp.bfloat16)

    def peer(i, y, sign, k):
        return lax.rem(z + (sign * OFFSETS[k][i]) % N_Z, jnp.int32(N_Z)) * N_YC + y

    def a_copy(k, i, y):
        return pltpu.make_async_remote_copy(
            src_ref=outb.at[k, i * N_YC + y],
            dst_ref=recv.at[k, i * N_YC + yc],
            send_sem=a_send.at[k],
            recv_sem=a_recv.at[k],
            device_id={"ep": peer(i, y, 1, k)},
            device_id_type=MESH,
        )

    def b_copy(k, i, y):
        return pltpu.make_async_remote_copy(
            src_ref=back.at[k, i * N_YC + y],
            dst_ref=ret.at[k, i * N_YC + yc],
            send_sem=b_send.at[k],
            recv_sem=b_recv.at[k],
            device_id={"ep": peer(i, y, -1, k)},
            device_id_type=MESH,
        )

    def spread(copy_of, k):
        def one(j, carry, halves):
            y = (yc + N_YC // 2 + j) & (N_YC - 1)
            for i in halves:
                if OFFSETS[k][i] == 0:

                    @pl.when(y != yc)
                    def _():
                        copy_of(k, i, y).start()
                else:
                    copy_of(k, i, y).start()
            return carry

        for halves in ((1,), (0,)) if k == SELF_CHUNK else ((0, 1),):
            lax.fori_loop(0, N_YC, functools.partial(one, halves=halves), 0)

    def bulk(buffer, sem, k):
        count = HALVES * N_YC - (k == SELF_CHUNK)
        view = buffer.at[k, pl.ds(0, count)]
        pltpu.make_async_copy(view, view, sem.at[k]).wait()

    def dispatch(k):
        row_id = lax.broadcasted_iota(jnp.int32, (ROWS, tok), 0) + k * ROWS
        hits = [row_id == s for s in slots]
        select = jnp.where(jnp.logical_or(hits[0], hits[1]), 1.0, 0.0).astype(jnp.bfloat16)
        shares = jnp.where(hits[0], weights_ref[0:1, :], 0.0) + jnp.where(
            hits[1], weights_ref[1:2, :], 0.0
        )
        coarse = shares.astype(jnp.bfloat16)
        mix[k, 0] = coarse
        mix[k, 1] = (shares - coarse.astype(jnp.float32)).astype(jnp.bfloat16)
        block = jnp.dot(select, row_ref[...], preferred_element_type=jnp.float32)
        tiles = rows_to_tiles(block.astype(jnp.bfloat16), perm_ref[...], width)
        flat = outb.at[k].reshape(ROWS, 16, lanes)
        for g in range(GROUPS):
            flat[16 * g : 16 * g + 16] = tiles[g]
        if k == SELF_CHUNK:
            recv[k, yc] = outb[k, yc]

    follower = lax.rem(me + 1, jnp.int32(N_Z * N_YC))

    def h_copy(which):
        ref = (keys_ref, values_ref)[which]
        return pltpu.make_async_remote_copy(
            src_ref=ref.at[:, pl.ds(ref.shape[1] - WINDOW, WINDOW)],
            dst_ref=halo.at[which],
            send_sem=h_send.at[which],
            recv_sem=h_recv.at[which],
            device_id={"ep": follower},
            device_id_type=MESH,
        )

    def begin():
        pl.semaphore_wait(barrier, n_ep - 1 + 2)
        h_copy(0).start()
        h_copy(1).start()

    def send(k):
        spread(a_copy, k)

    heads = queries_ref.shape[0] // HDIM
    sinks = jnp.concatenate(
        [jnp.broadcast_to(sink_ref[0:1, h : h + 1], (1, WINDOW)) for h in range(heads)], axis=1
    )
    key_i = lax.broadcasted_iota(jnp.int32, (2 * WINDOW, heads * WINDOW), 0)
    query_i = lax.broadcasted_iota(jnp.int32, (2 * WINDOW, heads * WINDOW), 1) & (WINDOW - 1)
    in_window = jnp.logical_and(key_i > query_i, key_i <= query_i + WINDOW)

    def attend(b, keys, values, allowed):
        at = slice(WINDOW * b, WINDOW * b + WINDOW)
        block = jnp.concatenate(
            [queries_ref[HDIM * h : HDIM * h + HDIM, at] for h in range(heads)], axis=1
        )
        scores = lax.dot_general(
            keys, block, (((0,), (0,)), ((), ())), preferred_element_type=jnp.float32
        ) * HDIM ** (-0.5)
        logits = jnp.where(allowed, scores, masked_value)
        top = jnp.maximum(jnp.max(logits, axis=0, keepdims=True), sinks)
        exponent = jnp.exp(logits - top)
        denominator = jnp.sum(exponent, axis=0, keepdims=True) + jnp.exp(sinks - top)
        probs = (exponent / denominator).astype(jnp.bfloat16)
        result = jnp.dot(values, probs, preferred_element_type=jnp.float32).astype(jnp.bfloat16)
        for h in range(heads):
            attended[HDIM * h : HDIM * h + HDIM, at] = result[:, WINDOW * h : WINDOW * h + WINDOW]

    blocks = queries_ref.shape[1] // WINDOW
    own_rows = mpart.shape[1]
    block_parts = WINDOW // own_rows

    def project(b):
        at_rows = slice(WINDOW * b, WINDOW * b + WINDOW)
        for n in range(width // 512):
            at = slice(512 * n, 512 * n + 512)
            part = lax.dot_general(
                attended[:, at_rows],
                wproj[:, at],
                (((0,), (0,)), ((), ())),
                preferred_element_type=jnp.float32,
            ).astype(jnp.bfloat16)
            mpart[block_parts * b : block_parts * b + block_parts, :, at] = part.reshape(
                block_parts, own_rows, 512
            )

    def mixer_own():
        for b in range(1, blocks):
            at = slice(WINDOW * (b - 1), WINDOW * (b + 1))
            attend(b, keys_ref[:, at], values_ref[:, at], in_window)
        pltpu.make_async_copy(wproj, wproj, w_sem.at[2]).wait()
        for b in range(1, blocks):
            project(b)

    def mixer_halo():
        with jax.named_scope("halo_wait"):
            h_copy(0).wait_recv()
            h_copy(1).wait_recv()
        first = slice(0, WINDOW)
        attend(
            0,
            jnp.concatenate([halo[0], keys_ref[:, first]], axis=1),
            jnp.concatenate([halo[1], values_ref[:, first]], axis=1),
            jnp.logical_and(in_window, jnp.logical_or(key_i >= WINDOW, me > 0)),
        )
        project(0)

    across = lax.rem(tp + 2, jnp.int32(n_tp))
    left_half = pl.ds(0, half)
    right_half = pl.ds(half, half)

    def m_copy(which):
        if which == 0:
            src, dst, to = mpart.at[across, :, left_half], m1.at[0], right
        elif which == 1:
            src, dst, to = mpart.at[across, :, right_half], m1.at[1], left
        elif which == 2:
            src, dst, to = mpart.at[right, :, right_half], m2.at[0, :, right_half], right
        elif which == 3:
            src, dst, to = mpart.at[left, :, left_half], m2.at[1, :, left_half], left
        elif which == 4:
            src, dst, to = mpart.at[right, :, left_half], m2.at[0, :, left_half], right
        else:
            src, dst, to = mpart.at[left, :, right_half], m2.at[1, :, right_half], left
        return pltpu.make_async_remote_copy(
            src_ref=src,
            dst_ref=dst,
            send_sem=m_send.at[which],
            recv_sem=m_recv.at[which],
            device_id={"tp": to},
            device_id_type=MESH,
        )

    def mixer_transit():
        m_copy(0).start()
        m_copy(1).start()

    def mixer_direct():
        m_copy(2).start()
        m_copy(3).start()

    def mixer_relay():
        m_copy(0).wait_recv()
        mpart[right, :, left_half] = (
            mpart[right, :, left_half].astype(jnp.float32) + m1[0].astype(jnp.float32)
        ).astype(jnp.bfloat16)
        m_copy(4).start()
        m_copy(1).wait_recv()
        mpart[left, :, right_half] = (
            mpart[left, :, right_half].astype(jnp.float32) + m1[1].astype(jnp.float32)
        ).astype(jnp.bfloat16)
        m_copy(5).start()

    def mixer_finish():
        for which in range(2, 6):
            m_copy(which).wait_recv()
        total = (
            mpart[tp].astype(jnp.float32)
            + m2[0].astype(jnp.float32)
            + m2[1].astype(jnp.float32)
        )
        squares = jnp.mean(total * total, axis=-1, keepdims=True)
        mixed_ref[...] = (total * lax.rsqrt(squares + norm_eps) * mix_gain_ref[...]).astype(
            jnp.bfloat16
        )

    low = pl.ds(0, half)
    high = pl.ds(half, half)

    def g_copy(k, which):
        if which == 0:
            src, dst, to = xbuf.at[k, 0], xbuf.at[k, 1], right
        elif which == 1:
            src, dst, to = xbuf.at[k, 0], xbuf.at[k, 2], left
        elif which == 2:
            src, dst, to = xbuf.at[k, 1, :, low], xbuf.at[k, 3, :, low], right
        else:
            src, dst, to = xbuf.at[k, 2, :, high], xbuf.at[k, 3, :, high], left
        return pltpu.make_async_remote_copy(
            src_ref=src,
            dst_ref=dst,
            send_sem=g_send.at[k, which],
            recv_sem=g_recv.at[k, which],
            device_id={"tp": to},
            device_id_type=MESH,
        )

    def q_copy(k, which):
        if which == 0:
            src, dst, to = pbuf.at[k, 3, :, low], r1.at[k, 0], right
        elif which == 1:
            src, dst, to = pbuf.at[k, 3, :, high], r1.at[k, 1], left
        elif which == 2:
            src, dst, to = pbuf.at[k, 2, :, high], r2.at[k, 0, :, high], right
        elif which == 3:
            src, dst, to = pbuf.at[k, 1, :, low], r2.at[k, 1, :, low], left
        elif which == 4:
            src, dst, to = pbuf.at[k, 2, :, low], r2.at[k, 0, :, low], right
        else:
            src, dst, to = pbuf.at[k, 1, :, high], r2.at[k, 1, :, high], left
        return pltpu.make_async_remote_copy(
            src_ref=src,
            dst_ref=dst,
            send_sem=q_send.at[k, which],
            recv_sem=q_recv.at[k, which],
            device_id={"tp": to},
            device_id_type=MESH,
        )

    def arrive(k):
        with jax.named_scope("arrive_wait"):
            bulk(recv, a_recv, k)
        rows = tiles_to_rows(recv[k].reshape(ROWS, 16, lanes), perm_ref[...], lanes)
        for g in range(GROUPS):
            for s in range(16):
                xbuf[k, 0, 16 * g : 16 * g + 16, lanes * s : lanes * s + lanes] = rows[g][s]
        g_copy(k, 0).start()
        g_copy(k, 1).start()

    def forward(k):
        with jax.named_scope("forward_wait"):
            g_copy(k, 0).wait_recv()
            g_copy(k, 2).start()
            g_copy(k, 1).wait_recv()
            g_copy(k, 3).start()

    def multiply(k, sends=True):
        if k == first_multiplied:
            pltpu.make_async_copy(wgu, wgu, w_sem.at[0]).wait()
            pltpu.make_async_copy(wdn, wdn, w_sem.at[1]).wait()

        with jax.named_scope("multiply_wait"):
            g_copy(k, 2).wait_recv()
            g_copy(k, 3).wait_recv()
        for n in range(gate_tiles):
            both = jnp.dot(
                xbuf[k].reshape(n_tp * ROWS, width), wgu[n], preferred_element_type=jnp.float32
            )
            gate, up = both[:, :128], both[:, 128:]
            hid[:, 128 * n : 128 * n + 128] = (gate / (1.0 + jnp.exp(-gate)) * up).astype(
                jnp.bfloat16
            )
        for n in range(down_tiles):
            part = jnp.dot(hid[...], wdn[n], preferred_element_type=jnp.float32)
            pbuf[k, :, :, 256 * n : 256 * n + 256] = part.astype(jnp.bfloat16).reshape(
                n_tp, ROWS, 256
            )
            if sends and n == down_tiles // 2 - 1:
                q_copy(k, 0).start()
        if sends:
            for which in range(1, 4):
                q_copy(k, which).start()

    def hand_on(k):
        for which in range(4):
            q_copy(k, which).start()

    def relay(k):
        with jax.named_scope("relay_wait"):
            q_copy(k, 0).wait_recv()
        pbuf[k, 2, :, low] = (
            pbuf[k, 2, :, low].astype(jnp.float32) + r1[k, 0].astype(jnp.float32)
        ).astype(jnp.bfloat16)
        q_copy(k, 4).start()
        q_copy(k, 1).wait_recv()
        pbuf[k, 1, :, high] = (
            pbuf[k, 1, :, high].astype(jnp.float32) + r1[k, 1].astype(jnp.float32)
        ).astype(jnp.bfloat16)
        q_copy(k, 5).start()

    def finish(k):
        with jax.named_scope("finish_wait"):
            for which in range(2, 6):
                q_copy(k, which).wait_recv()
        total = (
            pbuf[k, 0].astype(jnp.float32)
            + r2[k, 0].astype(jnp.float32)
            + r2[k, 1].astype(jnp.float32)
        ).astype(jnp.bfloat16)
        tiles = rows_to_tiles(total, perm_ref[...], width)
        flat = back.at[k].reshape(ROWS, 16, lanes)
        for g in range(GROUPS):
            flat[16 * g : 16 * g + 16] = tiles[g]
        if k == SELF_CHUNK:
            ret[k, yc] = back[k, yc]

        spread(b_copy, k)

    def combine(k):
        with jax.named_scope("combine_wait"):
            bulk(ret, b_recv, k)
        rows = tiles_to_rows(ret[k].reshape(ROWS, 16, lanes), perm_ref[...], lanes)
        block = jnp.concatenate([jnp.concatenate(r, axis=1) for r in rows], axis=0)
        dims = (((0,), (0,)), ((), ()))
        part = lax.dot_general(
            mix[k, 0], block, dims, preferred_element_type=jnp.float32
        ) + lax.dot_general(mix[k, 1], block, dims, preferred_element_type=jnp.float32)
        if k == last_combined:
            out_ref[...] = (acc[...] + part).astype(jnp.bfloat16)
        elif k == first_combined:
            acc[...] = part
        else:
            acc[...] += part

    stages = dict(
        D=dispatch,
        B=begin,
        S=send,
        O=mixer_own,
        H=mixer_halo,
        P=mixer_transit,
        Q=mixer_direct,
        R=mixer_relay,
        X=mixer_finish,
        A=arrive,
        F=forward,
        W=multiply,
        M=functools.partial(multiply, sends=False),
        T=hand_on,
        L=relay,
        E=finish,
        C=combine,
    )
    order = ORDER
    first_multiplied = [int(o[1]) for o in order if o[0] in "MW"][0]
    combined = [int(o[1]) for o in order if o[0] == "C"]
    first_combined, last_combined = combined[0], combined[-1]
    for op in order:
        with jax.named_scope(op):
            stages[op[0]](*(int(k) for k in op[1:]))

    def drain(k):
        bulk(outb, a_send, k)
        bulk(back, b_send, k)
        for which in range(4):
            g_copy(k, which).wait_send()
        for which in range(6):
            q_copy(k, which).wait_send()

    with jax.named_scope("drain"):
        for which in range(2):
            h_copy(which).wait_send()
        for which in range(6):
            m_copy(which).wait_send()
        for k in range(CHUNKS):
            drain(k)


def settle_kernel(mixed_ref, moe_ref, mixed_out, moe_out, sem):
    copies = [
        pltpu.make_async_copy(mixed_ref, mixed_out, sem.at[0]),
        pltpu.make_async_copy(moe_ref, moe_out, sem.at[1]),
    ]
    for copy in copies:
        copy.start()
    for copy in copies:
        copy.wait()


def settle(mixed, moe):
    hbm = pl.BlockSpec(memory_space=pl.ANY)
    vmem = pl.BlockSpec(memory_space=pltpu.VMEM)
    return pl.pallas_call(
        settle_kernel,
        out_shape=tuple(jax.ShapeDtypeStruct(a.shape, a.dtype) for a in (mixed, moe)),
        in_specs=[vmem, vmem],
        out_specs=(hbm, hbm),
        scratch_shapes=[pltpu.SemaphoreType.DMA((2,))],
        compiler_params=pltpu.CompilerParams(vmem_limit_bytes=58 * 1024 * 1024),
    )(*(pltpu.with_memory_space_constraint(a, pltpu.VMEM) for a in (mixed, moe)))


def shards(
    queries,
    key_rows,
    value_rows,
    sink_logits,
    out_weight,
    mix_gain,
    moe_tokens,
    moe_gain,
    routes,
    route_weights,
    expert_gate,
    expert_up,
    expert_down,
):
    tok, width = moe_tokens.shape
    n_tp = lax.axis_size("tp")
    hidden = expert_gate.shape[2]
    lanes = width // 16
    own_rows = queries.shape[0] // n_tp
    bf16 = jnp.bfloat16
    hbm = pl.BlockSpec(memory_space=pl.ANY)
    vmem = pl.BlockSpec(memory_space=pltpu.VMEM)
    dma = pltpu.SemaphoreType.DMA
    tiles = (CHUNKS, HALVES * N_YC, CAP, 16, lanes)
    small = (
        moe_tokens,
        moe_gain[None, :],
        routes.T,
        route_weights.T,
        queries.T,
        key_rows.T,
        value_rows.T,
        sink_logits[None, :],
        mix_gain[None, :],
    )
    mixed, moe = pl.pallas_call(
        functools.partial(layer_kernel, n_tp),
        out_shape=(pltpu.VMEM((own_rows, width), bf16), pltpu.VMEM((tok, width), bf16)),
        in_specs=[hbm] * 13,
        out_specs=(vmem, vmem),
        scratch_shapes=[
            *[pltpu.VMEM(a.shape, a.dtype) for a in small],
            pltpu.VMEM(tiles, bf16),
            pltpu.VMEM(tiles, bf16),
            pltpu.VMEM((CHUNKS, n_tp, ROWS, width), bf16),
            pltpu.VMEM((CHUNKS, n_tp, ROWS, width), bf16),
            pltpu.VMEM((CHUNKS, 2, ROWS, width // 2), bf16),
            pltpu.VMEM((CHUNKS, 2, ROWS, width), bf16),
            pltpu.VMEM(tiles, bf16),
            pltpu.VMEM(tiles, bf16),
            pltpu.VMEM((hidden // 128, width, 256), bf16),
            pltpu.VMEM((width // 256, hidden, 256), bf16),
            pltpu.VMEM((n_tp * ROWS, hidden), bf16),
            pltpu.VMEM((tok, width), jnp.float32),
            pltpu.VMEM((CHUNKS, 2, ROWS, tok), bf16),
            pltpu.VMEM((256, 256), bf16),
            pltpu.VMEM((tok, width), bf16),
            pltpu.VMEM((2, HDIM, WINDOW), bf16),
            pltpu.VMEM((queries.shape[1], queries.shape[0]), bf16),
            pltpu.VMEM(out_weight.shape, bf16),
            pltpu.VMEM((n_tp, own_rows, width), bf16),
            pltpu.VMEM((2, own_rows, width // 2), bf16),
            pltpu.VMEM((2, own_rows, width), bf16),
            dma((len(small),)),
            dma((2,)),
            dma((2,)),
            dma((6,)),
            dma((6,)),
            dma((3,)),
            dma((CHUNKS,)),
            dma((CHUNKS,)),
            dma((CHUNKS, 4)),
            dma((CHUNKS, 4)),
            dma((CHUNKS, 6)),
            dma((CHUNKS, 6)),
            dma((CHUNKS,)),
            dma((CHUNKS,)),
        ],
        compiler_params=pltpu.CompilerParams(
            collective_id=0, has_side_effects=True, vmem_limit_bytes=58 * 1024 * 1024
        ),
    )(*small, expert_gate, expert_up, expert_down, out_weight)
    return settle(mixed, moe)


def solution(mesh):
    return jax.shard_map(
        shards,
        mesh=mesh,
        in_specs=(
            P("ep", "tp"),
            P("ep", "tp"),
            P("ep", "tp"),
            P("tp"),
            P("tp", None),
            P(),
            P(("ep", "tp"), None),
            P(),
            P(("ep", "tp"), None),
            P(("ep", "tp"), None),
            P("ep", None, "tp"),
            P("ep", None, "tp"),
            P("ep", "tp", None),
        ),
        out_specs=(P(("ep", "tp"), None), P(("ep", "tp"), None)),
        check_vma=False,
    )
```
